512 devices in a mesh: kv: 64 (over z, y), tp: 8 (over x, core).
Axes of the slice: x: 4, y: 8, z: 8, core: 2. Of those that a mesh axis runs over, the one named last changes fastest.
Arguments:
- tokens: bfloat16 [128, 4096], P(None, 'kv'), may hold values from -16 to 16
- mix_gain: bfloat16 [4096], P('kv'), may hold values from 0.099609375 to 1.8984375
- ffn_gain: bfloat16 [4096], P('kv'), may hold values from 0.099609375 to 1.8984375
- w_query: bfloat16 [4096, 2048], P('kv', 'tp'), may hold values from -0.09375 to 0.09375
- w_key: bfloat16 [4096, 2048], P('kv', 'tp'), may hold values from -0.09375 to 0.09375
- w_value: bfloat16 [4096, 4096], P('kv', 'tp'), may hold values from -0.09375 to 0.09375
- w_gate: bfloat16 [4096, 4096], P('kv', 'tp'), may hold values from -0.09375 to 0.09375
- w_decay: bfloat16 [4096, 2048], P('kv', 'tp'), may hold values from -0.375 to 0.375
- decay_bias: float32 [2048], P('tp'), may hold values from -7 to 4
- head_gain: bfloat16 [512], replicated, may hold values from 0.099609375 to 1.8984375
- w_output: bfloat16 [4096, 4096], P('tp', 'kv'), may hold values from -0.09375 to 0.09375
- w_ffgate: bfloat16 [4096, 11008], P('kv', 'tp'), may hold values from -0.09375 to 0.09375
- w_ffup: bfloat16 [4096, 11008], P('kv', 'tp'), may hold values from -0.09375 to 0.09375
- w_down: bfloat16 [11008, 4096], P('tp', 'kv'), may hold values from -0.0546875 to 0.0546875
- state: float32 [128, 8, 256, 512], P('kv', 'tp'), may hold values from -6 to 6
Outputs:
- mixed: bfloat16 [128, 4096], P(None, 'kv')
- new_state: float32 [128, 8, 256, 512], P('kv', 'tp')
The draws below stay inside these ranges and needn't reach their ends.
All inputs are finite; a program needn't handle non-finite values.
Results may differ from the reference program's by a relative error of at most 0.015.
Values may be sent and summed in bfloat16 or wider, within the bound.
A program may use at most 64 MiB of HBM per device.

```python
import jax
import jax.numpy as jnp
from jax import lax

D = 4096
HEADS = 8
DK = 256
DV = 512
FF = 11008
SEQS = 128
GROUPS = 8


def draw_tokens(key, part):
    column = jnp.arange(D, dtype=jnp.float32) / D
    column_scale = 0.4 * jnp.exp(jnp.log(6.0) * column)
    values = jnp.clip(jax.random.normal(key, (SEQS, D), jnp.float32), -4.0, 4.0) * column_scale
    return values.astype(jnp.bfloat16)


def shard_levels(key, dims, pieces, least, largest):
    def one(dim, parts):
        steps = jax.random.uniform(jax.random.fold_in(jax.random.fold_in(key, 6), dim), (parts,), jnp.float32, least / len(pieces), largest / len(pieces))
        return jnp.repeat(jnp.exp(steps), dims[dim] // parts).reshape((-1,) + (1,) * (len(dims) - dim - 1))

    factor_of = one(*pieces[0])
    for cut in pieces[1:]:
        factor_of = factor_of * one(*cut)
    return factor_of


def normal_values(stream_key, extent, scale, reach, cuts=(), kind=jnp.bfloat16):
    values = jax.random.normal(stream_key, extent, jnp.float32) * scale
    if len(cuts) > 0:
        values = shard_levels(stream_key, extent, cuts, -0.22, 0.18) * values
    return jnp.clip(values, min=-reach, max=reach).astype(kind)


def setup_inputs(seed: int = 0) -> dict:
    key_of = jax.random.split(jax.random.key(seed), 16)
    tokens = draw_tokens(jax.random.fold_in(key_of[15], 71), 0)
    mix_gain = jnp.clip(1.0 + 0.18 * jax.random.normal(key_of[1], (D,), jnp.float32), 0.099609375, 1.8984375).astype(jnp.bfloat16)
    ffn_gain = jnp.clip(1.0 + 0.18 * jax.random.normal(key_of[2], (D,), jnp.float32), 0.099609375, 1.8984375).astype(jnp.bfloat16)
    w_query = normal_values(key_of[3], (D, HEADS * DK), D ** -0.5, 0.09375, ((0, 64), (1, 8)))
    w_key = normal_values(key_of[4], (D, HEADS * DK), D ** -0.5, 0.09375, ((0, 64), (1, 8)))
    w_value = normal_values(key_of[5], (D, HEADS * DV), D ** -0.5, 0.09375, ((0, 64), (1, 8)))
    w_gate = normal_values(key_of[6], (D, HEADS * DV), D ** -0.5, 0.09375, ((0, 64), (1, 8)))
    w_decay = normal_values(key_of[7], (D, HEADS * DK), (D // 16) ** -0.5, 0.375, ((0, 64), (1, 8)))
    decay_bias = jnp.clip(-7.0 + 11.0 * jax.random.uniform(key_of[8], (HEADS * DK,), jnp.float32) ** shard_levels(key_of[8], (HEADS * DK,), ((0, 8),), -0.2, 0.2), -7.0, 4.0)
    head_gain = jnp.clip(1.0 + 0.18 * jax.random.normal(key_of[9], (DV,), jnp.float32), 0.099609375, 1.8984375).astype(jnp.bfloat16)
    w_output = normal_values(key_of[10], (HEADS * DV, D), (HEADS * DV) ** -0.5, 0.09375, ((0, 8), (1, 64)))
    w_ffgate = normal_values(key_of[11], (D, FF), D ** -0.5, 0.09375, ((0, 64), (1, 8)))
    w_ffup = normal_values(key_of[12], (D, FF), D ** -0.5, 0.09375, ((0, 64), (1, 8)))
    w_down = normal_values(key_of[13], (FF, D), FF ** -0.5, 0.0546875, ((0, 8), (1, 64)))
    state = normal_values(key_of[14], (SEQS, HEADS, DK, DV), 1.0, 6.0, ((0, 64), (1, 8)), jnp.float32)
    return {"tokens": tokens, "mix_gain": mix_gain, "ffn_gain": ffn_gain, "w_query": w_query, "w_key": w_key, "w_value": w_value, "w_gate": w_gate, "w_decay": w_decay, "decay_bias": decay_bias, "head_gain": head_gain, "w_output": w_output, "w_ffgate": w_ffgate, "w_ffup": w_ffup, "w_down": w_down, "state": state}


epsilon = 1e-06

def reference(tokens, mix_gain, ffn_gain, w_query, w_key, w_value, w_gate, w_decay, decay_bias, head_gain, w_output, w_ffgate, w_ffup, w_down, state):
    seq_count = tokens.shape[0]
    model_width = tokens.shape[1]
    head_count = state.shape[1]
    key_dim = state.shape[2]
    val_dim = state.shape[3]
    token_f32 = tokens.astype(jnp.float32)
    mix_rms = lax.rsqrt(lax.optimization_barrier(jnp.sum(token_f32 * token_f32, axis=1)) / model_width + epsilon)[:, None]
    mix_in = (token_f32 * mix_gain.astype(jnp.float32)).astype(jnp.bfloat16)

    def project(weight):
        return jnp.dot(mix_in, weight, preferred_element_type=jnp.float32) * mix_rms
    queries = project(w_query).reshape(seq_count, head_count, key_dim) * key_dim ** (-0.5)
    key_rows = project(w_key).reshape(seq_count, head_count, key_dim)
    value_rows = project(w_value).reshape(seq_count, head_count, val_dim)
    gate_rows = project(w_gate).reshape(seq_count, head_count, val_dim)
    decay_rows = (project(w_decay) + decay_bias).reshape(seq_count, head_count, key_dim)
    log_decay = jax.nn.log_sigmoid(decay_rows) / 16.0
    new_state = jnp.exp(log_decay)[..., None] * state + key_rows[..., :, None] * value_rows[..., None, :]
    attended = jnp.einsum('bhk,bhkv->bhv', queries, new_state, precision=lax.Precision.HIGHEST)
    attended = attended * lax.rsqrt(lax.optimization_barrier(jnp.sum(attended * attended, axis=2, keepdims=True)) / val_dim + epsilon)
    head_out = (attended * head_gain.astype(jnp.float32) * jax.nn.silu(gate_rows)).reshape(seq_count, head_count * val_dim).astype(jnp.bfloat16)
    group_cols = head_count * val_dim // GROUPS
    attn_out = jnp.zeros((seq_count, model_width), jnp.float32)
    for group_idx in range(GROUPS):
        partial_value = jnp.dot(head_out[:, group_idx * group_cols:(group_idx + 1) * group_cols], w_output[group_idx * group_cols:(group_idx + 1) * group_cols], preferred_element_type=jnp.float32)
        attn_out = attn_out + lax.optimization_barrier(partial_value.astype(jnp.bfloat16)).astype(jnp.float32)
    residual_mid = (token_f32 + attn_out).astype(jnp.bfloat16)
    mid_f32 = residual_mid.astype(jnp.float32)
    ffn_rms = lax.rsqrt(lax.optimization_barrier(jnp.sum(mid_f32 * mid_f32, axis=1)) / model_width + epsilon)[:, None]
    ffn_in = (mid_f32 * ffn_gain.astype(jnp.float32)).astype(jnp.bfloat16)
    gate_sum = jnp.dot(ffn_in, w_ffgate, preferred_element_type=jnp.float32)
    up_sum = jnp.dot(ffn_in, w_ffup, preferred_element_type=jnp.float32)
    hidden = (jax.nn.silu(gate_sum * ffn_rms) * (up_sum * ffn_rms)).astype(jnp.bfloat16)
    unit_cols = hidden.shape[1] // GROUPS
    ffn_out = jnp.zeros((seq_count, model_width), jnp.float32)
    for group_idx in range(GROUPS):
        partial_value = jnp.dot(hidden[:, group_idx * unit_cols:(group_idx + 1) * unit_cols], w_down[group_idx * unit_cols:(group_idx + 1) * unit_cols], preferred_element_type=jnp.float32)
        ffn_out = ffn_out + lax.optimization_barrier(partial_value.astype(jnp.bfloat16)).astype(jnp.float32)
    mixed = (mid_f32 + ffn_out).astype(jnp.bfloat16)
    return (mixed, new_state)
```

```python
import jax
import jax.numpy as jnp
from jax import lax
from jax.experimental import pallas as pl
from jax.experimental.pallas import tpu as pltpu
from jax.sharding import PartitionSpec as P

MESH = pl.DeviceIdType.MESH
EPS = 1e-06
F32 = jnp.float32
BF16 = jnp.bfloat16
RING = 8
FAR_FIRST = (4, 3, 5, 2, 6, 1, 7)
Z_UNITS = 6
Y_UNITS = 5
UNITS = Z_UNITS + Y_UNITS
SKEW = 3


def far(k):
    odd = k % 2
    return (4 + (k // 2) * (1 - odd) - ((k + 1) // 2) * odd + RING) % RING


def wait_bytes(ref, sem):
    pltpu.make_async_copy(ref, ref, sem).wait()


def silu(v):
    return v / (1.0 + jnp.exp(-v))


def dot(a, b):
    return jnp.dot(a, b, preferred_element_type=F32)


def square_row(x):
    squares = x * x
    high = squares.astype(BF16)
    low = (squares - high.astype(F32)).astype(BF16)
    ones = jnp.ones((8, x.shape[1]), BF16)
    dims = (((1,), (1,)), ((), ()))
    total = lax.dot_general(ones, high, dims, preferred_element_type=F32)
    total = total + lax.dot_general(ones, low, dims, preferred_element_type=F32)
    return total[0:1, :]


def column_of(row, first, count):
    lane = lax.broadcasted_iota(jnp.int32, (count, row.shape[1]), 1)
    place = lax.broadcasted_iota(jnp.int32, (count, row.shape[1]), 0) + first
    return jnp.sum(jnp.where(lane == place, row, 0.0), axis=1, keepdims=True)


def kernel(
    tokens_h, mix_gain_h, ffn_gain_h, wq_h, wk_h, wv_h, wg_h, wd_h, bias_h, head_gain_h,
    wo_h, wfg_h, wfu_h, wdn_h, state_h,
    mixed_o, state_o,
    tokens_v, mix_gain_v, ffn_gain_v, w1_v, w2_v, bias_v, head_gain_v, wo_v, wfg_v, wfu_v, wdn_v, state_v,
    woa_v, wob_v, wgu_v, wda_v, wdb_v,
    az_s, az_r, ay_s, ay_r, az2_s, az2_r, ay2_s, ay2_r, ass_s, ass_r, ass2_s, ass2_r,
    b_s, b_r, c_s, c_r,
    dz_s, dz_r, dy_s, dy_r, dz2_s, dz2_r, dy2_s, dy2_r, dss_s, dss_r, dss2_s, dss2_r,
    e_s, e_r, f_s, f_r,
    in_sem, out_sem, send_sem, recv_sem,
):
    kv = lax.axis_index("kv")
    tp = lax.axis_index("tp")
    z = kv // RING
    y = kv % RING

    def at_z(d):
        return {"kv": ((z + d) % RING) * RING + y, "tp": tp}

    def at_y(d):
        return {"kv": z * RING + (y + d) % RING, "tp": tp}

    def at_tp(d):
        return {"kv": kv, "tp": (tp + d) % 8}

    barrier = pltpu.get_barrier_semaphore()
    for d in FAR_FIRST:
        for peer in (at_z(d), at_y(d), at_tp(d)):
            pl.semaphore_signal(barrier, inc=1, device_id=peer, device_id_type=MESH)

    def send(src, dst, slot, peer):
        pltpu.make_async_remote_copy(
            src_ref=src, dst_ref=dst, send_sem=send_sem.at[slot], recv_sem=recv_sem.at[slot],
            device_id=peer, device_id_type=MESH,
        ).start()

    loads = [
        (tokens_h, tokens_v), (mix_gain_h, mix_gain_v),
        (wq_h, w1_v.at[:, 0:256]), (wk_h, w1_v.at[:, 256:512]), (wd_h, w1_v.at[:, 512:768]),
        (wv_h.at[:, 0:128], w1_v.at[:, 768:896]), (wv_h.at[:, 128:512], w2_v.at[:, 0:384]),
        (wg_h, w2_v.at[:, 384:896]),
        (state_h, state_v), (bias_h, bias_v), (head_gain_h, head_gain_v), (ffn_gain_h, ffn_gain_v),
        (wo_h, wo_v), (wfg_h, wfg_v), (wfu_h, wfu_v), (wdn_h, wdn_v),
    ]
    copies = [pltpu.make_async_copy(src, dst, in_sem.at[n]) for n, (src, dst) in enumerate(loads)]
    for copy in copies:
        copy.start()
    for copy in copies[:8]:
        copy.wait()

    token_f32 = tokens_v[...].astype(F32)
    mix_in = (token_f32 * mix_gain_v[...].astype(F32)).astype(BF16)
    ass_s[0] = square_row(token_f32)
    az_s[...] = dot(mix_in, w1_v[...]).astype(BF16).reshape(az_s.shape)
    row = lax.broadcasted_iota(jnp.int32, (128, 128), 0)
    col = lax.broadcasted_iota(jnp.int32, (128, 128), 1)
    source = 16 * ((row % 16) // 2) + 2 * (row // 16) + row % 2
    shuffle = jnp.where(col == source, 1.0, 0.0).astype(BF16)
    mix_by_y = dot(shuffle, mix_in).astype(BF16)
    ay_s[...] = dot(mix_by_y, w2_v[...]).astype(BF16).reshape(ay_s.shape)

    pl.semaphore_wait(barrier, 21)
    for n, d in enumerate(FAR_FIRST):
        send(az_s.at[(z + d) % RING], az_r.at[d - 1], 0, at_z(d))
        send(ay_s.at[(y + d) % RING], ay_r.at[d - 1], 1, at_y(d))
        send(ass_s.at[0], ass_r.at[d - 1], 2, at_z(d))

    for copy in copies[8:]:
        copy.wait()
    zeros = jnp.zeros((512, 64), BF16)
    woa_v[...] = jnp.concatenate([wo_v[...], zeros], axis=1)
    wob_v[...] = jnp.concatenate([zeros, wo_v[...]], axis=1)
    rows = wdn_v.shape[0]
    zeros = jnp.zeros((rows, 64), BF16)
    wda_v[pl.ds(0, rows)] = jnp.concatenate([wdn_v[...], zeros], axis=1)
    wdb_v[pl.ds(0, rows)] = jnp.concatenate([zeros, wdn_v[...]], axis=1)
    wda_v[pl.ds(rows, 128 * UNITS - rows)] = jnp.zeros((128 * UNITS - rows, 128), BF16)
    wdb_v[pl.ds(rows, 128 * UNITS - rows)] = jnp.zeros((128 * UNITS - rows, 128), BF16)
    for u in range(UNITS):
        for side, ref in enumerate((wfg_v, wfu_v)):
            at = 256 * u + 128 * side
            width = min(128, ref.shape[1] - 128 * u)
            part = ref[:, 128 * u : 128 * u + width]
            if width < 128:
                part = jnp.concatenate([part, jnp.zeros((64, 128 - width), BF16)], axis=1)
            wgu_v[:, at : at + 128] = part

    wait_bytes(az_r, recv_sem.at[0])
    by_z = az_s[z].astype(F32)
    for n in range(7):
        by_z = by_z + az_r[n].astype(F32)
    by_z = by_z.astype(BF16)
    for n in range(RING):
        az2_s[n] = by_z[2 * n : 2 * n + 2, :]
    wait_bytes(ass_r, recv_sem.at[2])
    ss = ass_s[0]
    for n in range(7):
        ss = ss + ass_r[n]
    ass2_s[0] = ss
    for d in FAR_FIRST:
        send(az2_s.at[(y + d) % RING], az2_r.at[d - 1], 3, at_y(d))
        send(ass2_s.at[0], ass2_r.at[d - 1], 5, at_y(d))
    wait_bytes(ay_r, recv_sem.at[1])
    by_y = ay_s[y].astype(F32)
    for n in range(7):
        by_y = by_y + ay_r[n].astype(F32)
    by_y = by_y.astype(BF16)
    for n in range(RING):
        ay2_s[n] = by_y[2 * n : 2 * n + 2, :]
    for d in FAR_FIRST:
        send(ay2_s.at[(z + d) % RING], ay2_r.at[d - 1], 4, at_z(d))

    wait_bytes(az2_r, recv_sem.at[3])
    wait_bytes(ay2_r, recv_sem.at[4])
    wait_bytes(ass2_r, recv_sem.at[5])
    left = az2_s[y].astype(F32)
    right = ay2_s[z].astype(F32)
    ss = ass2_s[0]
    for n in range(7):
        left = left + az2_r[n].astype(F32)
        right = right + ay2_r[n].astype(F32)
        ss = ss + ass2_r[n]
    mix_rms = lax.rsqrt(column_of(ss, 2 * kv, 2) / 4096.0 + EPS)
    left = left * mix_rms
    right = right * mix_rms
    queries = left[:, 0:256] * (256.0 ** -0.5)
    keys = left[:, 256:512]
    raw_decay = left[:, 512:768] + bias_v[...]
    log_decay = (jnp.minimum(raw_decay, 0.0) - jnp.log1p(jnp.exp(-jnp.abs(raw_decay)))) / 16.0
    decay = jnp.exp(log_decay)
    values = jnp.concatenate([left[:, 768:896], right[:, 0:384]], axis=1)
    gates = right[:, 384:896]
    columns = jnp.concatenate([decay, keys, queries, queries], axis=0).T
    outs = []
    for s in range(2):
        value = values[s : s + 1, :]
        total = jnp.zeros((8, 512), F32)
        for block in range(8):
            rows = slice(32 * block, 32 * block + 32)
            fresh = columns[rows, s : s + 1] * state_v[s, rows, :] + columns[rows, 2 + s : 3 + s] * value
            state_v[s, rows, :] = fresh
            weighted = columns[rows, 4 + s : 5 + s] * fresh
            total = total + weighted[0:8] + weighted[8:16] + weighted[16:24] + weighted[24:32]
        outs.append(jnp.sum(total, axis=0, keepdims=True))
    state_out = pltpu.make_async_copy(state_v, state_o, out_sem.at[0])
    state_out.start()
    attended = jnp.concatenate(outs, axis=0)
    attended = attended * lax.rsqrt(jnp.sum(attended * attended, axis=1, keepdims=True) / 512.0 + EPS)
    head_out = (attended * head_gain_v[...].astype(F32) * silu(gates)).astype(BF16)
    b_s[0] = head_out
    b_r[kv] = head_out

    def spread_b(k, carry):
        peer = ((z + far(k // RING)) % RING) * RING + (y + far(k % RING)) % RING
        send(b_s.at[0], b_r.at[kv], 6, {"kv": peer, "tp": tp})
        return carry

    lax.fori_loop(0, 63, spread_b, 0)
    wait_bytes(b_r.at[pl.ds(0, 63)], recv_sem.at[6])
    heads = b_r[...].reshape(128, 512)
    partial = (dot(heads[0:64], woa_v[...]) + dot(heads[64:128], wob_v[...])).astype(BF16)
    c_s[0] = partial
    c_r[tp] = partial
    for d in (4, 3, 5, 2, 6, 1, 7):
        send(c_s.at[0], c_r.at[tp], 7, at_tp(d))
    token_pack = jnp.concatenate([token_f32[0:64], token_f32[64:128]], axis=1)
    gain_pack = jnp.concatenate([ffn_gain_v[...], ffn_gain_v[...]], axis=1).astype(F32)
    wait_bytes(c_r.at[pl.ds(0, 7)], recv_sem.at[7])
    attn_out = c_r[0].astype(F32)
    for n in range(1, 8):
        attn_out = attn_out + c_r[n].astype(F32)
    mid = (token_pack + attn_out).astype(BF16).astype(F32)
    ffn_pack = (mid * gain_pack).astype(BF16)
    ffn_in = jnp.concatenate([ffn_pack[:, 0:64], ffn_pack[:, 64:128]], axis=0)
    dss_s[0] = square_row(jnp.concatenate([mid[:, 0:64], mid[:, 64:128]], axis=0))
    for u in range(UNITS):
        part = dot(ffn_in, wgu_v[:, 256 * u : 256 * u + 256]).astype(BF16)
        for n in range(RING):
            block = part[16 * n : 16 * n + 16, :]
            if u < Z_UNITS:
                dz_s[n, u] = block
            else:
                dy_s[(SKEW * n + u - Z_UNITS - 2) % RING, u - Z_UNITS] = block
        if u == Z_UNITS - 1:
            for d in FAR_FIRST:
                send(dz_s.at[(z + d) % RING], dz_r.at[d - 1], 8, at_z(d))
                send(dss_s.at[0], dss_r.at[d - 1], 10, at_z(d))
    for d in FAR_FIRST:
        send(dy_s.at[(y + d) % RING], dy_r.at[d - 1], 9, at_y(d))

    wait_bytes(dss_r, recv_sem.at[10])
    ss = dss_s[0]
    for n in range(7):
        ss = ss + dss_r[n]
    dss2_s[0] = ss
    for d in FAR_FIRST:
        send(dss2_s.at[0], dss2_r.at[d - 1], 13, at_y(d))
    wait_bytes(dy_r, recv_sem.at[9])
    for j in range(Y_UNITS):
        part = dy_s[y, j].astype(F32)
        for n in range(7):
            part = part + dy_r[n, j].astype(F32)
        dy2_s[j] = part.astype(BF16)
    for d in FAR_FIRST:
        j = (y - SKEW * (z + d) + 2 + 64) % RING

        @pl.when(j < Y_UNITS)
        def _(j=j, d=d):
            send(dy2_s.at[j], dy2_r.at[d - 1], 12, at_z(d))

    wait_bytes(dz_r, recv_sem.at[8])
    for i in range(Z_UNITS):
        part = dz_s[z, i].astype(F32)
        for n in range(7):
            part = part + dz_r[n, i].astype(F32)
        dz2_s[i] = part.astype(BF16)
    for d in FAR_FIRST:
        i = (y + d - SKEW * z + 64) % RING

        @pl.when(i < Z_UNITS)
        def _(i=i, d=d):
            send(dz2_s.at[i], dz2_r.at[d - 1], 11, at_y(d))

    place = (y - SKEW * z + 64) % RING
    place_y = (place + 2) % RING
    wait_bytes(dss2_r, recv_sem.at[13])
    ss = dss2_s[0]
    for n in range(7):
        ss = ss + dss2_r[n]
    ffn_rms = lax.rsqrt(column_of(ss, 16 * z, 16) / 4096.0 + EPS)

    def finish(total, unit, slot):
        total = total * ffn_rms
        hidden = (silu(total[:, 0:128]) * total[:, 128:256]).astype(BF16)
        e_s[slot] = hidden
        e_r[unit * RING + z] = hidden

        def spread(k, carry):
            peer = ((z + far(k // RING)) % RING) * RING + (y + far(k % RING)) % RING
            send(e_s.at[slot], e_r.at[unit * RING + z], 14, {"kv": peer, "tp": tp})
            return carry

        lax.fori_loop(0, 63, spread, 0)

    @pl.when(place_y < Y_UNITS)
    def _():
        wait_bytes(dy2_r, recv_sem.at[12])
        total = dy2_s[place_y].astype(F32)
        for n in range(7):
            total = total + dy2_r[n].astype(F32)
        finish(total, Z_UNITS + place_y, 1)

    @pl.when(place < Z_UNITS)
    def _():
        wait_bytes(dz2_r, recv_sem.at[11])
        total = dz2_s[place].astype(F32)
        for n in range(7):
            total = total + dz2_r[n].astype(F32)
        finish(total, place, 0)

    one_only = (place // Z_UNITS) + (place_y // Y_UNITS)

    @pl.when(one_only == 0)
    def _():
        wait_bytes(e_r.at[pl.ds(0, 86)], recv_sem.at[14])

    @pl.when(one_only != 0)
    def _():
        wait_bytes(e_r.at[pl.ds(0, 87)], recv_sem.at[14])

    partial = jnp.zeros((64, 128), F32)
    for u in range(UNITS):
        block = e_r[8 * u : 8 * u + 8].reshape(128, 128)
        rows = slice(128 * u, 128 * u + 128)
        partial = partial + dot(block[0:64], wda_v[rows, :]) + dot(block[64:128], wdb_v[rows, :])
    partial = partial.astype(BF16)
    f_s[0] = partial
    f_r[tp] = partial
    for d in (4, 3, 5, 2, 6, 1, 7):
        send(f_s.at[0], f_r.at[tp], 15, at_tp(d))
    wait_bytes(f_r.at[pl.ds(0, 7)], recv_sem.at[15])
    ffn_out = f_r[0].astype(F32)
    for n in range(1, 8):
        ffn_out = ffn_out + f_r[n].astype(F32)
    out = (mid + ffn_out).astype(BF16)
    mixed_o[...] = jnp.concatenate([out[:, 0:64], out[:, 64:128]], axis=0)

    state_out.wait()
    for slot, ref in enumerate((az_r, ay_r, ass_r, az2_r, ay2_r, ass2_r, b_r.at[pl.ds(0, 63)], c_r.at[pl.ds(0, 7)], dz_r, dy_r, dss_r)):
        wait_bytes(ref, send_sem.at[slot])
    wait_bytes(dss2_r, send_sem.at[13])
    one = pl.ds(0, 1)
    for d in FAR_FIRST:

        @pl.when((y - SKEW * (z + d) + 2 + 64) % RING < Y_UNITS)
        def _():
            wait_bytes(dy2_r.at[one], send_sem.at[12])

        @pl.when((y + d - SKEW * z + 64) % RING < Z_UNITS)
        def _():
            wait_bytes(dz2_r.at[one], send_sem.at[11])

    @pl.when(place < Z_UNITS)
    def _():
        wait_bytes(e_r.at[pl.ds(0, 63)], send_sem.at[14])

    @pl.when(place_y < Y_UNITS)
    def _():
        wait_bytes(e_r.at[pl.ds(0, 63)], send_sem.at[14])

    wait_bytes(f_r.at[pl.ds(0, 7)], send_sem.at[15])


def local(
    tokens, mix_gain, ffn_gain, w_query, w_key, w_value, w_gate, w_decay, decay_bias, head_gain,
    w_output, w_ffgate, w_ffup, w_down, state,
):
    hidden_units = w_ffgate.shape[1]
    state = state.reshape(2, 256, 512)
    V = pltpu.VMEM
    scratch = [
        V((128, 64), BF16), V((1, 64), BF16), V((1, 64), BF16), V((64, 896), BF16), V((64, 896), BF16),
        V((1, 256), F32), V((1, 512), BF16), V((512, 64), BF16), V((64, hidden_units), BF16),
        V((64, hidden_units), BF16), V((hidden_units, 64), BF16), V((2, 256, 512), F32),
        V((512, 128), BF16), V((512, 128), BF16), V((64, 256 * UNITS), BF16),
        V((128 * UNITS, 128), BF16), V((128 * UNITS, 128), BF16),
        V((8, 16, 896), BF16), V((7, 16, 896), BF16), V((8, 16, 896), BF16), V((7, 16, 896), BF16),
        V((8, 2, 896), BF16), V((7, 2, 896), BF16), V((8, 2, 896), BF16), V((7, 2, 896), BF16),
        V((1, 1, 128), F32), V((7, 1, 128), F32), V((1, 1, 128), F32), V((7, 1, 128), F32),
        V((1, 2, 512), BF16), V((64, 2, 512), BF16), V((1, 64, 128), BF16), V((8, 64, 128), BF16),
        V((8, Z_UNITS, 16, 256), BF16), V((7, Z_UNITS, 16, 256), BF16),
        V((8, Y_UNITS, 16, 256), BF16), V((7, Y_UNITS, 16, 256), BF16),
        V((Z_UNITS, 16, 256), BF16), V((7, 16, 256), BF16), V((Y_UNITS, 16, 256), BF16), V((7, 16, 256), BF16),
        V((1, 1, 128), F32), V((7, 1, 128), F32), V((1, 1, 128), F32), V((7, 1, 128), F32),
        V((2, 16, 128), BF16), V((8 * UNITS, 16, 128), BF16), V((1, 64, 128), BF16), V((8, 64, 128), BF16),
        pltpu.SemaphoreType.DMA((16,)), pltpu.SemaphoreType.DMA((1,)),
        pltpu.SemaphoreType.DMA((16,)), pltpu.SemaphoreType.DMA((16,)),
    ]
    mixed, new_state = pl.pallas_call(
        kernel,
        name="layer",
        out_shape=(
            jax.ShapeDtypeStruct((128, 64), BF16),
            jax.ShapeDtypeStruct((2, 256, 512), F32),
        ),
        in_specs=[pl.BlockSpec(memory_space=pl.ANY)] * 15,
        out_specs=(pl.BlockSpec(memory_space=pltpu.VMEM), pl.BlockSpec(memory_space=pl.ANY)),
        scratch_shapes=scratch,
        compiler_params=pltpu.CompilerParams(
            collective_id=0, has_side_effects=True, vmem_limit_bytes=60 * 2**20
        ),
    )(
        tokens, mix_gain.reshape(1, 64), ffn_gain.reshape(1, 64), w_query, w_key, w_value, w_gate, w_decay,
        decay_bias.reshape(1, 256), head_gain.reshape(1, 512), w_output, w_ffgate, w_ffup, w_down, state,
    )
    return (mixed, new_state.reshape(2, 1, 256, 512))


def solution(mesh):
    in_specs = (
        P(None, "kv"),
        P("kv"),
        P("kv"),
        P("kv", "tp"),
        P("kv", "tp"),
        P("kv", "tp"),
        P("kv", "tp"),
        P("kv", "tp"),
        P("tp"),
        P(),
        P("tp", "kv"),
        P("kv", "tp"),
        P("kv", "tp"),
        P("tp", "kv"),
        P("kv", "tp", None, None),
    )
    out_specs = (P(None, "kv"), P("kv", "tp", None, None))
    return jax.shard_map(local, mesh=mesh, in_specs=in_specs, out_specs=out_specs, check_vma=False)
```

```python
import jax
import jax.numpy as jnp
from jax import lax
from jax.experimental import pallas as pl
from jax.experimental.pallas import tpu as pltpu
from jax.sharding import PartitionSpec as P

MESH = pl.DeviceIdType.MESH
EPS = 1e-06
F32 = jnp.float32
BF16 = jnp.bfloat16
RING = 8
FAR_FIRST = (4, 3, 5, 2, 6, 1, 7)
UNITS = 11


def far(k):
    odd = k % 2
    return (4 + (k // 2) * (1 - odd) - ((k + 1) // 2) * odd + RING) % RING


def wait_bytes(ref, sem):
    pltpu.make_async_copy(ref, ref, sem).wait()


def silu(v):
    return v / (1.0 + jnp.exp(-v))


def dot(a, b):
    return jnp.dot(a, b, preferred_element_type=F32)


def dot_nt(a, b):
    return lax.dot_general(a, b, (((1,), (1,)), ((), ())), preferred_element_type=F32)


def square_row(x):
    squares = x * x
    high = squares.astype(BF16)
    low = (squares - high.astype(F32)).astype(BF16)
    ones = jnp.ones((8, x.shape[0]), BF16)
    return (dot(ones, high) + dot(ones, low))[0:1, :]


def column_of(row, first, count):
    lane = lax.broadcasted_iota(jnp.int32, (count, row.shape[1]), 1)
    place = lax.broadcasted_iota(jnp.int32, (count, row.shape[1]), 0) + first
    return jnp.sum(jnp.where(lane == place, row, 0.0), axis=1, keepdims=True)


def kernel(
    tokens_h, mix_gain_h, ffn_gain_h, wq_h, wk_h, wv_h, wg_h, wd_h, bias_h, head_gain_h,
    wo_h, wfg_h, wfu_h, wdn_h, state_h,
    mixed_o, rows_o,
    tokens_v, mix_gain_v, ffn_gain_v, w1_v, w2_v, bias_v, head_gain_v, wo_v, wfg_v, wfu_v, wdn_v, state_v,
    wgu_v, wlast_v,
    az_s, az_r, ay_s, ay_r, az2_s, az2_r, ay2_s, ay2_r, ass_s, ass_r, ass2_s, ass2_r,
    b_s, b_r, c_s, c_r,
    w_r, x_s, x_r, d_s, d_r, dss_s, dss_r, dss2_s, dss2_r,
    e_s, e_r, f_s, f_r,
    in_sem, send_sem, recv_sem,
):
    kv = lax.axis_index("kv")
    tp = lax.axis_index("tp")
    z = kv // RING
    y = kv % RING

    def at_z(d):
        return {"kv": ((z + d) % RING) * RING + y, "tp": tp}

    def at_y(d):
        return {"kv": z * RING + (y + d) % RING, "tp": tp}

    def at_tp(d):
        return {"kv": kv, "tp": (tp + d) % 8}

    def send(src, dst, slot, peer):
        pltpu.make_async_remote_copy(
            src_ref=src, dst_ref=dst, send_sem=send_sem.at[slot], recv_sem=recv_sem.at[slot],
            device_id=peer, device_id_type=MESH,
        ).start()

    loads = [
        (tokens_h, tokens_v), (mix_gain_h, mix_gain_v),
        (wq_h, w1_v.at[:, 0:256]), (wk_h, w1_v.at[:, 256:512]), (wd_h, w1_v.at[:, 512:768]),
        (wv_h.at[:, 0:128], w1_v.at[:, 768:896]), (wv_h.at[:, 128:512], w2_v.at[:, 0:384]),
        (wg_h, w2_v.at[:, 384:896]),
        (state_h, state_v), (bias_h, bias_v), (head_gain_h, head_gain_v), (ffn_gain_h, ffn_gain_v),
        (wo_h, wo_v), (wfg_h, wfg_v), (wfu_h, wfu_v), (wdn_h, wdn_v),
    ]
    copies = [pltpu.make_async_copy(src, dst, in_sem.at[n]) for n, (src, dst) in enumerate(loads)]
    for copy in copies:
        copy.start()
    barrier = pltpu.get_barrier_semaphore()
    for d in FAR_FIRST:
        for peer in (at_z(d), at_y(d), at_tp(d)):
            pl.semaphore_signal(barrier, inc=1, device_id=peer, device_id_type=MESH)

    for copy in copies[:6]:
        copy.wait()

    token_f32 = tokens_v[...].astype(F32)
    mix_t = (token_f32 * column_of(mix_gain_v[...].astype(F32), 0, 64)).astype(BF16)
    row = lax.broadcasted_iota(jnp.int32, (128, 128), 0)
    col = lax.broadcasted_iota(jnp.int32, (128, 128), 1)
    keep = jnp.where(col == row, 1.0, 0.0).astype(BF16)
    by_y = 16 * ((row % 16) // 2) + 2 * (row // 16) + row % 2
    shuffle = jnp.where(col == by_y, 1.0, 0.0).astype(BF16)
    mix_in = dot_nt(keep, mix_t).astype(BF16)
    az_s[...] = dot(mix_in, w1_v[...]).astype(BF16).reshape(az_s.shape)
    ass_s[0] = square_row(token_f32)

    pl.semaphore_wait(barrier, 21)
    for d in FAR_FIRST:
        send(az_s.at[(z + d) % RING], az_r.at[d - 1], 0, at_z(d))
    for copy in copies[6:8]:
        copy.wait()
    mix_by_y = dot_nt(shuffle, mix_t).astype(BF16)
    ay_s[...] = dot(mix_by_y, w2_v[...]).astype(BF16).reshape(ay_s.shape)
    for d in FAR_FIRST:
        send(ay_s.at[(y + d) % RING], ay_r.at[d - 1], 1, at_y(d))
    for d in FAR_FIRST:
        send(ass_s.at[0], ass_r.at[d - 1], 2, at_z(d))

    for copy in copies[8:]:
        copy.wait()
    last = wdn_v.shape[1] % 128
    wlast_v[...] = jnp.concatenate([wdn_v[:, 128 * UNITS - 128 :], jnp.zeros((64, 128 - last), BF16)], axis=1)
    for u in range(UNITS):
        for side, ref in enumerate((wfg_v, wfu_v)):
            width = min(128, ref.shape[1] - 128 * u)
            part = ref[:, 128 * u : 128 * u + width]
            if width < 128:
                part = jnp.concatenate([part, jnp.zeros((64, 128 - width), BF16)], axis=1)
            wgu_v[u, :, 128 * side : 128 * side + 128] = part
    w_r[0, y] = wgu_v[y]
    w_r[1, y] = wgu_v[8 + y // 3]

    wait_bytes(az_r, recv_sem.at[0])
    by_z = az_s[z].astype(F32)
    for n in range(7):
        by_z = by_z + az_r[n].astype(F32)
    by_z = by_z.astype(BF16)
    for n in range(RING):
        az2_s[n] = by_z[2 * n : 2 * n + 2, :]
    wait_bytes(ass_r, recv_sem.at[2])
    ss = ass_s[0]
    for n in range(7):
        ss = ss + ass_r[n]
    ass2_s[0] = ss
    for d in FAR_FIRST:
        send(az2_s.at[(y + d) % RING], az2_r.at[d - 1], 3, at_y(d))
        send(ass2_s.at[0], ass2_r.at[d - 1], 5, at_y(d))
    wait_bytes(ay_r, recv_sem.at[1])
    by_y = ay_s[y].astype(F32)
    for n in range(7):
        by_y = by_y + ay_r[n].astype(F32)
    by_y = by_y.astype(BF16)
    for n in range(RING):
        ay2_s[n] = by_y[2 * n : 2 * n + 2, :]
    for d in FAR_FIRST:
        send(ay2_s.at[(z + d) % RING], ay2_r.at[d - 1], 4, at_z(d))
    for d in FAR_FIRST:
        send(wgu_v.at[(y + d) % RING], w_r.at[0, y], 8, at_y(d))

    wait_bytes(az2_r, recv_sem.at[3])
    wait_bytes(ay2_r, recv_sem.at[4])
    wait_bytes(ass2_r, recv_sem.at[5])
    left = az2_s[y].astype(F32)
    right = ay2_s[z].astype(F32)
    ss = ass2_s[0]
    for n in range(7):
        left = left + az2_r[n].astype(F32)
        right = right + ay2_r[n].astype(F32)
        ss = ss + ass2_r[n]
    mix_rms = lax.rsqrt(column_of(ss, 2 * kv, 2) / 4096.0 + EPS)
    left = left * mix_rms
    right = right * mix_rms
    queries = left[:, 0:256] * (256.0 ** -0.5)
    keys = left[:, 256:512]
    raw_decay = left[:, 512:768] + bias_v[...]
    log_decay = (jnp.minimum(raw_decay, 0.0) - jnp.log1p(jnp.exp(-jnp.abs(raw_decay)))) / 16.0
    decay = jnp.exp(log_decay)
    values = jnp.concatenate([left[:, 768:896], right[:, 0:384]], axis=1)
    gates = right[:, 384:896]
    rows_o[:, 0:256] = decay
    rows_o[:, 256:512] = keys
    rows_o[:, 512:1024] = values
    columns = jnp.concatenate([decay, keys, queries, queries], axis=0).T
    outs = []
    for s in range(2):
        value = values[s : s + 1, :]
        total = jnp.zeros((8, 512), F32)
        for block in range(8):
            rows = slice(32 * block, 32 * block + 32)
            fresh = columns[rows, s : s + 1] * state_v[s, rows, :] + columns[rows, 2 + s : 3 + s] * value
            weighted = columns[rows, 4 + s : 5 + s] * fresh
            total = total + weighted[0:8] + weighted[8:16] + weighted[16:24] + weighted[24:32]
        outs.append(jnp.sum(total, axis=0, keepdims=True))
    attended = jnp.concatenate(outs, axis=0)
    attended = attended * lax.rsqrt(jnp.sum(attended * attended, axis=1, keepdims=True) / 512.0 + EPS)
    head_out = (attended * head_gain_v[...].astype(F32)[None, :] * silu(gates)).astype(BF16)
    b_s[0] = head_out
    b_r[kv] = head_out

    def spread_b(k, carry):
        peer = ((z + far(k // RING)) % RING) * RING + (y + far(k % RING)) % RING
        send(b_s.at[0], b_r.at[kv], 6, {"kv": peer, "tp": tp})
        return carry

    lax.fori_loop(0, 63, spread_b, 0)
    wait_bytes(b_r.at[pl.ds(0, 63)], recv_sem.at[6])
    heads = b_r[...].reshape(128, 512)
    partial = dot_nt(wo_v[...], heads).astype(BF16)
    c_s[0] = partial
    c_r[tp] = partial
    for d in (4, 3, 5, 2, 6, 1, 7):
        send(c_s.at[0], c_r.at[tp], 7, at_tp(d))
    for d in FAR_FIRST:

        @pl.when((y + d) % RING % 3 == 0)
        def _(d=d):
            send(wgu_v.at[8 + (y + d) % RING // 3], w_r.at[1, y], 9, at_y(d))

    gain_column = column_of(ffn_gain_v[...].astype(F32), 0, 64)
    wait_bytes(c_r.at[pl.ds(0, 7)], recv_sem.at[7])
    attn_out = c_r[0].astype(F32)
    for n in range(1, 8):
        attn_out = attn_out + c_r[n].astype(F32)
    mid = (token_f32 + attn_out).astype(BF16).astype(F32)
    ffn_in = (mid * gain_column).astype(BF16)
    x_s[0] = ffn_in
    x_r[y] = ffn_in
    for d in FAR_FIRST:
        send(x_s.at[0], x_r.at[y], 10, at_y(d))
    dss_s[0] = square_row(mid)
    for d in FAR_FIRST:
        send(dss_s.at[0], dss_r.at[d - 1], 11, at_y(d))

    second = y % 3 == 0
    wait_bytes(w_r.at[0, pl.ds(0, 7)], recv_sem.at[8])
    wait_bytes(x_r.at[pl.ds(0, 7)], recv_sem.at[10])
    rows_in = dot_nt(keep, x_r[...].reshape(512, 128)).astype(BF16)
    d_s[0] = dot(rows_in, w_r[0].reshape(512, 256)).astype(BF16).reshape(8, 16, 256)
    for d in FAR_FIRST:
        send(d_s.at[0, (z + d) % RING], d_r.at[0, d - 1], 12, at_z(d))

    @pl.when(second)
    def _():
        wait_bytes(w_r.at[1, pl.ds(0, 7)], recv_sem.at[9])
        d_s[1] = dot(rows_in, w_r[1].reshape(512, 256)).astype(BF16).reshape(8, 16, 256)
        for d in FAR_FIRST:
            send(d_s.at[1, (z + d) % RING], d_r.at[1, d - 1], 13, at_z(d))

    wait_bytes(dss_r, recv_sem.at[11])
    ss = dss_s[0]
    for n in range(7):
        ss = ss + dss_r[n]
    dss2_s[0] = ss
    for d in FAR_FIRST:
        send(dss2_s.at[0], dss2_r.at[d - 1], 14, at_z(d))
    wait_bytes(dss2_r, recv_sem.at[14])
    for n in range(7):
        ss = ss + dss2_r[n]
    ffn_rms = lax.rsqrt(column_of(ss, 16 * z, 16) / 4096.0 + EPS)

    def finish(unit, slot):
        wait_bytes(d_r.at[slot], recv_sem.at[12 + slot])
        total = d_s[slot, z].astype(F32)
        for n in range(7):
            total = total + d_r[slot, n].astype(F32)
        total = total * ffn_rms
        hidden = (silu(total[:, 0:128]) * total[:, 128:256]).astype(BF16)
        e_s[slot] = hidden
        e_r[unit * RING + z] = hidden

        def spread(k, carry):
            peer = ((z + far(k // RING)) % RING) * RING + (y + far(k % RING)) % RING
            send(e_s.at[slot], e_r.at[unit * RING + z], 15, {"kv": peer, "tp": tp})
            return carry

        lax.fori_loop(0, 63, spread, 0)

    @pl.when(second)
    def _():
        finish(8 + y // 3, 1)

    finish(y, 0)

    @pl.when(second)
    def _():
        wait_bytes(e_r.at[pl.ds(0, 86)], recv_sem.at[15])

    @pl.when(jnp.logical_not(second))
    def _():
        wait_bytes(e_r.at[pl.ds(0, 87)], recv_sem.at[15])

    hidden = jnp.concatenate([e_r[8 * u : 8 * u + 8].reshape(128, 128) for u in range(UNITS)], axis=1)
    weight = jnp.concatenate([wdn_v[:, 0 : 128 * UNITS - 128], wlast_v[...]], axis=1)
    partial = dot_nt(weight, hidden).astype(BF16)
    f_s[0] = partial
    f_r[tp] = partial
    for d in (4, 3, 5, 2, 6, 1, 7):
        send(f_s.at[0], f_r.at[tp], 16, at_tp(d))
    wait_bytes(f_r.at[pl.ds(0, 7)], recv_sem.at[16])
    ffn_out = f_r[0].astype(F32)
    for n in range(1, 8):
        ffn_out = ffn_out + f_r[n].astype(F32)
    mixed_o[...] = (mid + ffn_out).astype(BF16)

    seven = pl.ds(0, 7)
    drains = (
        az_r, ay_r, ass_r, az2_r, ay2_r, ass2_r, b_r.at[pl.ds(0, 63)], c_r.at[seven], w_r.at[0, seven], None,
        x_r.at[seven], dss_r, d_r.at[0], None, dss2_r, e_r.at[pl.ds(0, 63)], f_r.at[seven],
    )
    for slot, ref in enumerate(drains):
        if ref is not None:
            wait_bytes(ref, send_sem.at[slot])

    @pl.when(second)
    def _():
        wait_bytes(d_r.at[1], send_sem.at[13])
        wait_bytes(e_r.at[pl.ds(0, 63)], send_sem.at[15])

    for d in FAR_FIRST:

        @pl.when((y + d) % RING % 3 == 0)
        def _():
            wait_bytes(w_r.at[1, pl.ds(0, 1)], send_sem.at[9])


def local(
    tokens, mix_gain, ffn_gain, w_query, w_key, w_value, w_gate, w_decay, decay_bias, head_gain,
    w_output, w_ffgate, w_ffup, w_down, state,
):
    hidden_units = w_ffgate.shape[1]
    V = pltpu.VMEM
    scratch = [
        V((64, 128), BF16), V((1, 64), BF16), V((1, 64), BF16), V((64, 896), BF16), V((64, 896), BF16),
        V((1, 256), F32), V((512,), BF16), V((64, 512), BF16), V((64, hidden_units), BF16),
        V((64, hidden_units), BF16), V((64, hidden_units), BF16), V((2, 256, 512), F32),
        V((UNITS, 64, 256), BF16), V((64, 128), BF16),
        V((8, 16, 896), BF16), V((7, 16, 896), BF16), V((8, 16, 896), BF16), V((7, 16, 896), BF16),
        V((8, 2, 896), BF16), V((7, 2, 896), BF16), V((8, 2, 896), BF16), V((7, 2, 896), BF16),
        V((1, 1, 128), F32), V((7, 1, 128), F32), V((1, 1, 128), F32), V((7, 1, 128), F32),
        V((1, 2, 512), BF16), V((64, 2, 512), BF16), V((1, 64, 128), BF16), V((8, 64, 128), BF16),
        V((2, 8, 64, 256), BF16), V((1, 64, 128), BF16), V((8, 64, 128), BF16),
        V((2, 8, 16, 256), BF16), V((2, 7, 16, 256), BF16),
        V((1, 1, 128), F32), V((7, 1, 128), F32), V((1, 1, 128), F32), V((7, 1, 128), F32),
        V((2, 16, 128), BF16), V((8 * UNITS, 16, 128), BF16), V((1, 64, 128), BF16), V((8, 64, 128), BF16),
        pltpu.SemaphoreType.DMA((16,)),
        pltpu.SemaphoreType.DMA((17,)), pltpu.SemaphoreType.DMA((17,)),
    ]
    mixed, rows = pl.pallas_call(
        kernel,
        name="layer",
        out_shape=(
            jax.ShapeDtypeStruct((64, 128), BF16),
            jax.ShapeDtypeStruct((2, 1024), F32),
        ),
        in_specs=[pl.BlockSpec(memory_space=pltpu.HBM)] * 15,
        out_specs=[pl.BlockSpec(memory_space=pltpu.VMEM)] * 2,
        scratch_shapes=scratch,
        compiler_params=pltpu.CompilerParams(
            collective_id=0, has_side_effects=True, vmem_limit_bytes=64000000
        ),
    )(
        tokens.T, mix_gain.reshape(1, 64), ffn_gain.reshape(1, 64), w_query, w_key, w_value, w_gate, w_decay,
        decay_bias.reshape(1, 256), head_gain, w_output.T, w_ffgate, w_ffup, w_down.T, state.reshape(2, 256, 512),
    )
    decay, key, value = (rows[:, 0:256], rows[:, 256:512], rows[:, 512:1024])
    new_state = decay[:, None, :, None] * state + key[:, None, :, None] * value[:, None, None, :]
    return (mixed.T, new_state)


def solution(mesh):
    in_specs = (
        P(None, "kv"),
        P("kv"),
        P("kv"),
        P("kv", "tp"),
        P("kv", "tp"),
        P("kv", "tp"),
        P("kv", "tp"),
        P("kv", "tp"),
        P("tp"),
        P(),
        P("tp", "kv"),
        P("kv", "tp"),
        P("kv", "tp"),
        P("tp", "kv"),
        P("kv", "tp", None, None),
    )
    out_specs = (P(None, "kv"), P("kv", "tp", None, None))
    return jax.shard_map(local, mesh=mesh, in_specs=in_specs, out_specs=out_specs, check_vma=False)
```

```python
import jax
import jax.numpy as jnp
from jax import lax
from jax.experimental import pallas as pl
from jax.experimental.pallas import tpu as pltpu
from jax.sharding import PartitionSpec as P

MESH = pl.DeviceIdType.MESH
EPS = 1e-06
F32 = jnp.float32
BF16 = jnp.bfloat16
RING = 8
FAR_FIRST = (4, 3, 5, 2, 6, 1, 7)
UNITS = 11


def far(k):
    odd = k % 2
    return (4 + (k // 2) * (1 - odd) - ((k + 1) // 2) * odd + RING) % RING


def wait_bytes(ref, sem):
    pltpu.make_async_copy(ref, ref, sem).wait()


def silu(v):
    return v / (1.0 + jnp.exp(-v))


def dot(a, b):
    return jnp.dot(a, b, preferred_element_type=F32)


def dot_nt(a, b):
    return lax.dot_general(a, b, (((1,), (1,)), ((), ())), preferred_element_type=F32)


def square_row(x):
    squares = x * x
    high = squares.astype(BF16)
    low = (squares - high.astype(F32)).astype(BF16)
    ones = jnp.ones((8, x.shape[0]), BF16)
    return (dot(ones, high) + dot(ones, low))[0:1, :]


def column_of(row, first, count):
    lane = lax.broadcasted_iota(jnp.int32, (count, row.shape[1]), 1)
    place = lax.broadcasted_iota(jnp.int32, (count, row.shape[1]), 0) + first
    return jnp.sum(jnp.where(lane == place, row, 0.0), axis=1, keepdims=True)


def kernel(
    tokens_h, mix_gain_h, ffn_gain_h, wq_h, wk_h, wv_h, wg_h, wd_h, bias_h, head_gain_h,
    wo_h, wfg_h, wfu_h, wdn_h, state_h,
    mixed_o, decay_o, key_o, value_o,
    tokens_v, mix_gain_v, ffn_gain_v, w1_v, w2_v, bias_v, head_gain_v, wo_v, wfg_v, wfu_v, wdn_v, state_v,
    wgu_v, wdt_v,
    az_s, az_r, ay_s, ay_r, az2_s, az2_r, ay2_s, ay2_r, ass_s, ass_r, ass2_s, ass2_r,
    b_s, b_r, c_s, c_r,
    w_r, x_s, x_r, d_s, d_r, dss_s, dss_r, dss2_s, dss2_r,
    v_r, e_s, e_r, g_s, g_r, f_s, f_r,
    in_sem, send_sem, recv_sem,
):
    kv = lax.axis_index("kv")
    tp = lax.axis_index("tp")
    z = kv // RING
    y = kv % RING

    def at_z(d):
        return {"kv": ((z + d) % RING) * RING + y, "tp": tp}

    def at_y(d):
        return {"kv": z * RING + (y + d) % RING, "tp": tp}

    def at_tp(d):
        return {"kv": kv, "tp": (tp + d) % 8}

    def send(src, dst, slot, peer):
        pltpu.make_async_remote_copy(
            src_ref=src, dst_ref=dst, send_sem=send_sem.at[slot], recv_sem=recv_sem.at[slot],
            device_id=peer, device_id_type=MESH,
        ).start()

    loads = [
        (tokens_h, tokens_v), (mix_gain_h, mix_gain_v),
        (wq_h, w1_v.at[:, 0:256]), (wk_h, w1_v.at[:, 256:512]), (wd_h, w1_v.at[:, 512:768]),
        (wv_h.at[:, 0:128], w1_v.at[:, 768:896]), (wv_h.at[:, 128:512], w2_v.at[:, 0:384]),
        (wg_h, w2_v.at[:, 384:896]),
        (state_h, state_v), (bias_h, bias_v), (head_gain_h, head_gain_v), (ffn_gain_h, ffn_gain_v),
        (wo_h, wo_v), (wfg_h, wfg_v), (wfu_h, wfu_v), (wdn_h, wdn_v),
    ]
    copies = [pltpu.make_async_copy(src, dst, in_sem.at[n]) for n, (src, dst) in enumerate(loads)]
    for copy in copies:
        copy.start()
    barrier = pltpu.get_barrier_semaphore()
    for d in FAR_FIRST:
        for peer in (at_z(d), at_y(d), at_tp(d)):
            pl.semaphore_signal(barrier, inc=1, device_id=peer, device_id_type=MESH)

    for copy in copies[:6]:
        copy.wait()

    token_f32 = tokens_v[...].astype(F32)
    mix_t = (token_f32 * column_of(mix_gain_v[...].astype(F32), 0, 64)).astype(BF16)
    row = lax.broadcasted_iota(jnp.int32, (128, 128), 0)
    col = lax.broadcasted_iota(jnp.int32, (128, 128), 1)
    keep = jnp.where(col == row, 1.0, 0.0).astype(BF16)
    by_y = 16 * ((row % 16) // 2) + 2 * (row // 16) + row % 2
    shuffle = jnp.where(col == by_y, 1.0, 0.0).astype(BF16)
    mix_in = dot_nt(keep, mix_t).astype(BF16)
    az_s[...] = dot(mix_in, w1_v[...]).astype(BF16).reshape(az_s.shape)
    ass_s[0] = square_row(token_f32)

    pl.semaphore_wait(barrier, 21)
    for d in FAR_FIRST:
        send(az_s.at[(z + d) % RING], az_r.at[d - 1], 0, at_z(d))
    for copy in copies[6:8]:
        copy.wait()
    mix_by_y = dot_nt(shuffle, mix_t).astype(BF16)
    ay_s[...] = dot(mix_by_y, w2_v[...]).astype(BF16).reshape(ay_s.shape)
    for d in FAR_FIRST:
        send(ay_s.at[(y + d) % RING], ay_r.at[d - 1], 1, at_y(d))
    for d in FAR_FIRST:
        send(ass_s.at[0], ass_r.at[d - 1], 2, at_z(d))

    for copy in copies[8:]:
        copy.wait()
    for u in range(UNITS):
        for side, ref in enumerate((wfg_v, wfu_v, wdn_v)):
            width = min(128, ref.shape[1] - 128 * u)
            part = ref[:, 128 * u : 128 * u + width]
            if width < 128:
                part = jnp.concatenate([part, jnp.zeros((64, 128 - width), BF16)], axis=1)
            if side < 2:
                wgu_v[u, :, 128 * side : 128 * side + 128] = part
            else:
                wdt_v[u] = part
    w_r[0, y] = wgu_v[y]
    w_r[1, y] = wgu_v[8 + y // 3]
    v_r[0, y] = wdt_v[y]
    v_r[1, y] = wdt_v[8 + y // 3]

    wait_bytes(az_r, recv_sem.at[0])
    by_z = az_s[z].astype(F32)
    for n in range(7):
        by_z = by_z + az_r[n].astype(F32)
    by_z = by_z.astype(BF16)
    for n in range(RING):
        az2_s[n] = by_z[2 * n : 2 * n + 2, :]
    wait_bytes(ass_r, recv_sem.at[2])
    ss = ass_s[0]
    for n in range(7):
        ss = ss + ass_r[n]
    ass2_s[0] = ss
    for d in FAR_FIRST:
        send(az2_s.at[(y + d) % RING], az2_r.at[d - 1], 3, at_y(d))
        send(ass2_s.at[0], ass2_r.at[d - 1], 5, at_y(d))
    wait_bytes(ay_r, recv_sem.at[1])
    by_y = ay_s[y].astype(F32)
    for n in range(7):
        by_y = by_y + ay_r[n].astype(F32)
    by_y = by_y.astype(BF16)
    for n in range(RING):
        ay2_s[n] = by_y[2 * n : 2 * n + 2, :]
    for d in FAR_FIRST:
        send(ay2_s.at[(z + d) % RING], ay2_r.at[d - 1], 4, at_z(d))
    for d in FAR_FIRST:
        send(wgu_v.at[(y + d) % RING], w_r.at[0, y], 8, at_y(d))

    wait_bytes(az2_r, recv_sem.at[3])
    wait_bytes(ay2_r, recv_sem.at[4])
    wait_bytes(ass2_r, recv_sem.at[5])
    left = az2_s[y].astype(F32)
    right = ay2_s[z].astype(F32)
    ss = ass2_s[0]
    for n in range(7):
        left = left + az2_r[n].astype(F32)
        right = right + ay2_r[n].astype(F32)
        ss = ss + ass2_r[n]
    mix_rms = lax.rsqrt(column_of(ss, 2 * kv, 2) / 4096.0 + EPS)
    left = left * mix_rms
    right = right * mix_rms
    queries = left[:, 0:256] * (256.0 ** -0.5)
    keys = left[:, 256:512]
    raw_decay = left[:, 512:768] + bias_v[...]
    log_decay = (jnp.minimum(raw_decay, 0.0) - jnp.log1p(jnp.exp(-jnp.abs(raw_decay)))) / 16.0
    decay = jnp.exp(log_decay)
    values = jnp.concatenate([left[:, 768:896], right[:, 0:384]], axis=1)
    gates = right[:, 384:896]
    decay_o[...] = decay
    key_o[...] = keys
    value_o[...] = values
    columns = jnp.concatenate([decay, keys, queries, queries], axis=0).T
    outs = []
    for s in range(2):
        value = values[s : s + 1, :]
        total = jnp.zeros((8, 512), F32)
        for block in range(8):
            rows = slice(32 * block, 32 * block + 32)
            fresh = columns[rows, s : s + 1] * state_v[s, rows, :] + columns[rows, 2 + s : 3 + s] * value
            weighted = columns[rows, 4 + s : 5 + s] * fresh
            total = total + weighted[0:8] + weighted[8:16] + weighted[16:24] + weighted[24:32]
        outs.append(jnp.sum(total, axis=0, keepdims=True))
    attended = jnp.concatenate(outs, axis=0)
    attended = attended * lax.rsqrt(jnp.sum(attended * attended, axis=1, keepdims=True) / 512.0 + EPS)
    head_out = (attended * head_gain_v[...].astype(F32)[None, :] * silu(gates)).astype(BF16)
    b_s[0] = head_out
    b_r[kv] = head_out

    def spread_b(k, carry):
        peer = ((z + far(k // RING)) % RING) * RING + (y + far(k % RING)) % RING
        send(b_s.at[0], b_r.at[kv], 6, {"kv": peer, "tp": tp})
        return carry

    lax.fori_loop(0, 63, spread_b, 0)
    wait_bytes(b_r.at[pl.ds(0, 63)], recv_sem.at[6])
    heads = b_r[...].reshape(128, 512)
    partial = dot_nt(wo_v[...], heads).astype(BF16)
    c_s[0] = partial
    c_r[tp] = partial
    for d in (4, 3, 5, 2, 6, 1, 7):
        send(c_s.at[0], c_r.at[tp], 7, at_tp(d))
    for d in FAR_FIRST:

        @pl.when((y + d) % RING % 3 == 0)
        def _(d=d):
            send(wgu_v.at[8 + (y + d) % RING // 3], w_r.at[1, y], 9, at_y(d))

    gain_column = column_of(ffn_gain_v[...].astype(F32), 0, 64)
    wait_bytes(c_r.at[pl.ds(0, 7)], recv_sem.at[7])
    attn_out = c_r[0].astype(F32)
    for n in range(1, 8):
        attn_out = attn_out + c_r[n].astype(F32)
    mid = (token_f32 + attn_out).astype(BF16).astype(F32)
    ffn_in = (mid * gain_column).astype(BF16)
    x_s[0] = ffn_in
    x_r[y] = ffn_in
    for d in FAR_FIRST:
        send(x_s.at[0], x_r.at[y], 10, at_y(d))
    dss_s[0] = square_row(mid)
    for d in FAR_FIRST:
        send(dss_s.at[0], dss_r.at[d - 1], 11, at_y(d))

    second = y % 3 == 0
    wait_bytes(w_r.at[0, pl.ds(0, 7)], recv_sem.at[8])
    wait_bytes(x_r.at[pl.ds(0, 7)], recv_sem.at[10])
    rows_in = dot_nt(keep, x_r[...].reshape(512, 128)).astype(BF16)
    d_s[0] = dot(rows_in, w_r[0].reshape(512, 256)).astype(BF16).reshape(8, 16, 256)
    for d in FAR_FIRST:
        send(d_s.at[0, (z + d) % RING], d_r.at[0, d - 1], 12, at_z(d))

    @pl.when(second)
    def _():
        wait_bytes(w_r.at[1, pl.ds(0, 7)], recv_sem.at[9])
        d_s[1] = dot(rows_in, w_r[1].reshape(512, 256)).astype(BF16).reshape(8, 16, 256)
        for d in FAR_FIRST:
            send(d_s.at[1, (z + d) % RING], d_r.at[1, d - 1], 13, at_z(d))

    for d in FAR_FIRST:
        send(wdt_v.at[(y + d) % RING], v_r.at[0, y], 18, at_y(d))

        @pl.when((y + d) % RING % 3 == 0)
        def _(d=d):
            send(wdt_v.at[8 + (y + d) % RING // 3], v_r.at[1, y], 19, at_y(d))

    wait_bytes(dss_r, recv_sem.at[11])
    ss = dss_s[0]
    for n in range(7):
        ss = ss + dss_r[n]
    dss2_s[0] = ss
    for d in FAR_FIRST:
        send(dss2_s.at[0], dss2_r.at[d - 1], 14, at_z(d))
    wait_bytes(dss2_r, recv_sem.at[14])
    for n in range(7):
        ss = ss + dss2_r[n]
    ffn_rms = lax.rsqrt(column_of(ss, 16 * z, 16) / 4096.0 + EPS)

    def finish(slot):
        wait_bytes(d_r.at[slot], recv_sem.at[12 + slot])
        total = d_s[slot, z].astype(F32)
        for n in range(7):
            total = total + d_r[slot, n].astype(F32)
        total = total * ffn_rms
        hidden = (silu(total[:, 0:128]) * total[:, 128:256]).astype(BF16)
        e_s[slot] = hidden
        e_r[slot, z] = hidden
        for d in FAR_FIRST:
            send(e_s.at[slot], e_r.at[slot, z], 15 + slot, at_z(d))

    @pl.when(second)
    def _():
        finish(1)

    finish(0)

    def down(slot):
        wait_bytes(e_r.at[slot, pl.ds(0, 7)], recv_sem.at[15 + slot])
        wait_bytes(v_r.at[slot, pl.ds(0, 7)], recv_sem.at[18 + slot])
        return dot_nt(v_r[slot].reshape(512, 128), e_r[slot].reshape(128, 128))

    @pl.when(second)
    def _():
        g_s[...] = (down(1) + down(0)).astype(BF16).reshape(8, 64, 128)

    @pl.when(jnp.logical_not(second))
    def _():
        g_s[...] = down(0).astype(BF16).reshape(8, 64, 128)

    for d in FAR_FIRST:
        send(g_s.at[(y + d) % RING], g_r.at[d - 1], 20, at_y(d))
    wait_bytes(g_r, recv_sem.at[20])
    partial = g_s[y].astype(F32)
    for n in range(7):
        partial = partial + g_r[n].astype(F32)
    partial = partial.astype(BF16)
    f_s[0] = partial
    f_r[tp] = partial
    for d in (4, 3, 5, 2, 6, 1, 7):
        send(f_s.at[0], f_r.at[tp], 17, at_tp(d))
    wait_bytes(f_r.at[pl.ds(0, 7)], recv_sem.at[17])
    ffn_out = f_r[0].astype(F32)
    for n in range(1, 8):
        ffn_out = ffn_out + f_r[n].astype(F32)
    mixed_o[...] = (mid + ffn_out).astype(BF16)

    seven = pl.ds(0, 7)
    drains = (
        az_r, ay_r, ass_r, az2_r, ay2_r, ass2_r, b_r.at[pl.ds(0, 63)], c_r.at[seven], w_r.at[0, seven], None,
        x_r.at[seven], dss_r, d_r.at[0], None, dss2_r, e_r.at[0, seven], None, f_r.at[seven],
        v_r.at[0, seven], None, g_r,
    )
    for slot, ref in enumerate(drains):
        if ref is not None:
            wait_bytes(ref, send_sem.at[slot])

    @pl.when(second)
    def _():
        wait_bytes(d_r.at[1], send_sem.at[13])
        wait_bytes(e_r.at[1, seven], send_sem.at[16])

    for d in FAR_FIRST:

        @pl.when((y + d) % RING % 3 == 0)
        def _():
            wait_bytes(w_r.at[1, pl.ds(0, 1)], send_sem.at[9])
            wait_bytes(v_r.at[1, pl.ds(0, 1)], send_sem.at[19])


def local(
    tokens, mix_gain, ffn_gain, w_query, w_key, w_value, w_gate, w_decay, decay_bias, head_gain,
    w_output, w_ffgate, w_ffup, w_down, state,
):
    hidden_units = w_ffgate.shape[1]
    V = pltpu.VMEM
    scratch = [
        V((64, 128), BF16), V((1, 64), BF16), V((1, 64), BF16), V((64, 896), BF16), V((64, 896), BF16),
        V((1, 256), F32), V((512,), BF16), V((64, 512), BF16), V((64, hidden_units), BF16),
        V((64, hidden_units), BF16), V((64, hidden_units), BF16), V((2, 256, 512), F32),
        V((UNITS, 64, 256), BF16), V((UNITS, 64, 128), BF16),
        V((8, 16, 896), BF16), V((7, 16, 896), BF16), V((8, 16, 896), BF16), V((7, 16, 896), BF16),
        V((8, 2, 896), BF16), V((7, 2, 896), BF16), V((8, 2, 896), BF16), V((7, 2, 896), BF16),
        V((1, 1, 128), F32), V((7, 1, 128), F32), V((1, 1, 128), F32), V((7, 1, 128), F32),
        V((1, 2, 512), BF16), V((64, 2, 512), BF16), V((1, 64, 128), BF16), V((8, 64, 128), BF16),
        V((2, 8, 64, 256), BF16), V((1, 64, 128), BF16), V((8, 64, 128), BF16),
        V((2, 8, 16, 256), BF16), V((2, 7, 16, 256), BF16),
        V((1, 1, 128), F32), V((7, 1, 128), F32), V((1, 1, 128), F32), V((7, 1, 128), F32),
        V((2, 8, 64, 128), BF16), V((2, 16, 128), BF16), V((2, 8, 16, 128), BF16), V((8, 64, 128), BF16), V((7, 64, 128), BF16), V((1, 64, 128), BF16), V((8, 64, 128), BF16),
        pltpu.SemaphoreType.DMA((16,)),
        pltpu.SemaphoreType.DMA((21,)), pltpu.SemaphoreType.DMA((21,)),
    ]
    operands = (
        tokens.T, mix_gain.reshape(1, 64), ffn_gain.reshape(1, 64), w_query, w_key, w_value, w_gate, w_decay,
        decay_bias.reshape(1, 256), head_gain, w_output.T, w_ffgate, w_ffup, w_down.T, state.reshape(2, 256, 512),
    )
    mixed, decay, key, value = pl.pallas_call(
        kernel,
        name="layer",
        out_shape=(
            jax.ShapeDtypeStruct((64, 128), BF16),
            jax.ShapeDtypeStruct((2, 256), F32),
            jax.ShapeDtypeStruct((2, 256), F32),
            jax.ShapeDtypeStruct((2, 512), F32),
        ),
        in_specs=[pl.BlockSpec(memory_space=pltpu.HBM)] * 15,
        out_specs=[pl.BlockSpec(memory_space=pltpu.VMEM)] * 4,
        scratch_shapes=scratch,
        compiler_params=pltpu.CompilerParams(
            collective_id=0, has_side_effects=True, vmem_limit_bytes=40000000
        ),
    )(*[pltpu.with_memory_space_constraint(a, pltpu.HBM) for a in operands])
    new_state = decay[:, None, :, None] * state + key[:, None, :, None] * value[:, None, None, :]
    return (mixed.T, new_state)


def solution(mesh):
    in_specs = (
        P(None, "kv"),
        P("kv"),
        P("kv"),
        P("kv", "tp"),
        P("kv", "tp"),
        P("kv", "tp"),
        P("kv", "tp"),
        P("kv", "tp"),
        P("tp"),
        P(),
        P("tp", "kv"),
        P("kv", "tp"),
        P("kv", "tp"),
        P("tp", "kv"),
        P("kv", "tp", None, None),
    )
    out_specs = (P(None, "kv"), P("kv", "tp", None, None))
    return jax.shard_map(local, mesh=mesh, in_specs=in_specs, out_specs=out_specs, check_vma=False)
```

```python
import jax
import jax.numpy as jnp
from jax import lax
from jax.experimental import pallas as pl
from jax.experimental.pallas import tpu as pltpu
from jax.sharding import PartitionSpec as P

MESH = pl.DeviceIdType.MESH
EPS = 1e-06
F32 = jnp.float32
BF16 = jnp.bfloat16
RING = 8
FAR_FIRST = (4, 3, 5, 2, 6, 1, 7)
UNITS = 11
SPREAD = sorted(
    ((dz, dy) for dz in range(RING) for dy in range(RING) if dz + dy > 0),
    key=lambda t: -min(t[0], RING - t[0]) - min(t[1], RING - t[1]),
)


def far(k):
    odd = k % 2
    return (4 + (k // 2) * (1 - odd) - ((k + 1) // 2) * odd + RING) % RING


def wait_bytes(ref, sem):
    pltpu.make_async_copy(ref, ref, sem).wait()


def silu(v):
    return v / (1.0 + jnp.exp(-v))


def dot(a, b):
    return jnp.dot(a, b, preferred_element_type=F32)


def dot_nt(a, b):
    return lax.dot_general(a, b, (((1,), (1,)), ((), ())), preferred_element_type=F32)


def square_row(x):
    squares = x * x
    high = squares.astype(BF16)
    low = (squares - high.astype(F32)).astype(BF16)
    ones = jnp.ones((8, x.shape[0]), BF16)
    return (dot(ones, high) + dot(ones, low))[0:1, :]


def column_of(row, first, count):
    lane = lax.broadcasted_iota(jnp.int32, (count, row.shape[1]), 1)
    place = lax.broadcasted_iota(jnp.int32, (count, row.shape[1]), 0) + first
    return jnp.sum(jnp.where(lane == place, row, 0.0), axis=1, keepdims=True)


def kernel(
    tokens_h, mix_gain_h, ffn_gain_h, wq_h, wk_h, wv_h, wg_h, wd_h, bias_h, head_gain_h,
    wo_h, wfg_h, wfu_h, wdn_h, state_h,
    mixed_o, state_v,
    tokens_v, mix_gain_v, ffn_gain_v, w1_v, w2_v, bias_v, head_gain_v, wo_v, wfg_v, wfu_v, wdn_v,
    wgu_v, wdt_v,
    az_s, az_r, ay_s, ay_r, az2_s, az2_r, ay2_s, ay2_r, ass_s, ass_r, ass2_s, ass2_r,
    b_s, b_r, c_s, c_r,
    w_r, x_s, x_r, d_s, d_r, dss_s, dss_r, dss2_s, dss2_r,
    v_r, e_s, e_r, g_s, g_r, f_s, f_r,
    in_sem, send_sem, recv_sem,
):
    kv = lax.axis_index("kv")
    tp = lax.axis_index("tp")
    z = kv // RING
    y = kv % RING

    def at_z(d):
        return {"kv": ((z + d) % RING) * RING + y, "tp": tp}

    def at_y(d):
        return {"kv": z * RING + (y + d) % RING, "tp": tp}

    def at_tp(d):
        return {"kv": kv, "tp": (tp + d) % 8}

    def send(src, dst, slot, peer):
        pltpu.make_async_remote_copy(
            src_ref=src, dst_ref=dst, send_sem=send_sem.at[slot], recv_sem=recv_sem.at[slot],
            device_id=peer, device_id_type=MESH,
        ).start()

    loads = [
        (tokens_h, tokens_v), (mix_gain_h, mix_gain_v),
        (wq_h, w1_v.at[:, 0:256]), (wk_h, w1_v.at[:, 256:512]), (wd_h, w1_v.at[:, 512:768]),
        (wv_h.at[:, 0:128], w1_v.at[:, 768:896]), (wv_h.at[:, 128:512], w2_v.at[:, 0:384]),
        (wg_h, w2_v.at[:, 384:896]),
        (state_h, state_v), (bias_h, bias_v), (head_gain_h, head_gain_v), (ffn_gain_h, ffn_gain_v),
        (wo_h, wo_v), (wfg_h, wfg_v), (wfu_h, wfu_v), (wdn_h, wdn_v),
    ]
    copies = [pltpu.make_async_copy(src, dst, in_sem.at[n]) for n, (src, dst) in enumerate(loads)]
    for copy in copies:
        copy.start()
    barrier = pltpu.get_barrier_semaphore()
    for d in FAR_FIRST:
        for peer in (at_z(d), at_y(d), at_tp(d)):
            pl.semaphore_signal(barrier, inc=1, device_id=peer, device_id_type=MESH)

    for copy in copies[:6]:
        copy.wait()

    token_f32 = tokens_v[...].astype(F32)
    mix_t = (token_f32 * column_of(mix_gain_v[...].astype(F32), 0, 64)).astype(BF16)
    row = lax.broadcasted_iota(jnp.int32, (128, 128), 0)
    col = lax.broadcasted_iota(jnp.int32, (128, 128), 1)
    keep = jnp.where(col == row, 1.0, 0.0).astype(BF16)
    by_y = 16 * ((row % 16) // 2) + 2 * (row // 16) + row % 2
    shuffle = jnp.where(col == by_y, 1.0, 0.0).astype(BF16)
    mix_in = dot_nt(keep, mix_t).astype(BF16)
    az_s[...] = dot(mix_in, w1_v[...]).astype(BF16).reshape(az_s.shape)
    ass_s[0] = square_row(token_f32)

    for copy in copies[6:8]:
        copy.wait()
    mix_by_y = dot_nt(shuffle, mix_t).astype(BF16)
    ay_s[...] = dot(mix_by_y, w2_v[...]).astype(BF16).reshape(ay_s.shape)
    pl.semaphore_wait(barrier, 21)
    for d in FAR_FIRST:
        send(az_s.at[(z + d) % RING], az_r.at[d - 1], 0, at_z(d))
        send(ay_s.at[(y + d) % RING], ay_r.at[d - 1], 1, at_y(d))
    for d in FAR_FIRST:
        send(ass_s.at[0], ass_r.at[d - 1], 2, at_z(d))

    for copy in copies[8:]:
        copy.wait()
    for u in range(UNITS):
        for side, ref in enumerate((wfg_v, wfu_v, wdn_v)):
            width = min(128, ref.shape[1] - 128 * u)
            part = ref[:, 128 * u : 128 * u + width]
            if width < 128:
                part = jnp.concatenate([part, jnp.zeros((64, 128 - width), BF16)], axis=1)
            if side < 2:
                wgu_v[u, :, 128 * side : 128 * side + 128] = part
            else:
                wdt_v[u] = part
    w_r[0, y] = wgu_v[y]
    w_r[1, y] = wgu_v[8 + y // 3]
    v_r[0, y] = wdt_v[y]
    v_r[1, y] = wdt_v[8 + y // 3]

    wait_bytes(az_r, recv_sem.at[0])
    by_z = az_s[z].astype(F32)
    for n in range(7):
        by_z = by_z + az_r[n].astype(F32)
    by_z = by_z.astype(BF16)
    for n in range(RING):
        az2_s[n] = by_z[2 * n : 2 * n + 2, :]
    wait_bytes(ass_r, recv_sem.at[2])
    ss = ass_s[0]
    for n in range(7):
        ss = ss + ass_r[n]
    ass2_s[0] = ss
    for d in FAR_FIRST:
        send(az2_s.at[(y + d) % RING], az2_r.at[d - 1], 3, at_y(d))
        send(ass2_s.at[0], ass2_r.at[d - 1], 5, at_y(d))
    wait_bytes(ay_r, recv_sem.at[1])
    by_y = ay_s[y].astype(F32)
    for n in range(7):
        by_y = by_y + ay_r[n].astype(F32)
    by_y = by_y.astype(BF16)
    for n in range(RING):
        ay2_s[n] = by_y[2 * n : 2 * n + 2, :]
    for d in FAR_FIRST:
        send(ay2_s.at[(z + d) % RING], ay2_r.at[d - 1], 4, at_z(d))
    for d in FAR_FIRST:
        send(wgu_v.at[(y + d) % RING], w_r.at[0, y], 8, at_y(d))

    wait_bytes(az2_r, recv_sem.at[3])
    wait_bytes(ay2_r, recv_sem.at[4])
    wait_bytes(ass2_r, recv_sem.at[5])
    left = az2_s[y].astype(F32)
    right = ay2_s[z].astype(F32)
    ss = ass2_s[0]
    for n in range(7):
        left = left + az2_r[n].astype(F32)
        right = right + ay2_r[n].astype(F32)
        ss = ss + ass2_r[n]
    mix_rms = lax.rsqrt(column_of(ss, 2 * kv, 2) / 4096.0 + EPS)
    left = left * mix_rms
    right = right * mix_rms
    queries = left[:, 0:256] * (256.0 ** -0.5)
    keys = left[:, 256:512]
    raw_decay = left[:, 512:768] + bias_v[...]
    log_decay = (jnp.minimum(raw_decay, 0.0) - jnp.log1p(jnp.exp(-jnp.abs(raw_decay)))) / 16.0
    decay = jnp.exp(log_decay)
    values = jnp.concatenate([left[:, 768:896], right[:, 0:384]], axis=1)
    gates = right[:, 384:896]
    columns = jnp.concatenate([decay, keys, queries, queries], axis=0).T
    outs = []
    for s in range(2):
        value = values[s : s + 1, :]
        total = jnp.zeros((8, 512), F32)
        for block in range(8):
            rows = slice(32 * block, 32 * block + 32)
            fresh = columns[rows, s : s + 1] * state_v[s, rows, :] + columns[rows, 2 + s : 3 + s] * value
            state_v[s, rows, :] = fresh
            weighted = columns[rows, 4 + s : 5 + s] * fresh
            total = total + weighted[0:8] + weighted[8:16] + weighted[16:24] + weighted[24:32]
        outs.append(jnp.sum(total, axis=0, keepdims=True))
    attended = jnp.concatenate(outs, axis=0)
    attended = attended * lax.rsqrt(jnp.sum(attended * attended, axis=1, keepdims=True) / 512.0 + EPS)
    head_out = (attended * head_gain_v[...].astype(F32)[None, :] * silu(gates)).astype(BF16)
    b_s[0] = head_out
    b_r[kv] = head_out

    for dz, dy in SPREAD:
        peer = ((z + dz) % RING) * RING + (y + dy) % RING
        send(b_s.at[0], b_r.at[kv], 6, {"kv": peer, "tp": tp})
    wait_bytes(b_r.at[pl.ds(0, 63)], recv_sem.at[6])
    heads = b_r[...].reshape(128, 512)
    partial = dot_nt(wo_v[...], heads).astype(BF16)
    c_s[0] = partial
    c_r[tp] = partial
    for d in (4, 3, 5, 2, 6, 1, 7):
        send(c_s.at[0], c_r.at[tp], 7, at_tp(d))
    for d in FAR_FIRST:

        @pl.when((y + d) % RING % 3 == 0)
        def _(d=d):
            send(wgu_v.at[8 + (y + d) % RING // 3], w_r.at[1, y], 9, at_y(d))

    gain_column = column_of(ffn_gain_v[...].astype(F32), 0, 64)
    wait_bytes(c_r.at[pl.ds(0, 7)], recv_sem.at[7])
    attn_out = c_r[0].astype(F32)
    for n in range(1, 8):
        attn_out = attn_out + c_r[n].astype(F32)
    mid = (token_f32 + attn_out).astype(BF16).astype(F32)
    ffn_in = (mid * gain_column).astype(BF16)
    x_s[0] = ffn_in
    x_r[y] = ffn_in
    for d in FAR_FIRST:
        send(x_s.at[0], x_r.at[y], 10, at_y(d))
    dss_s[0] = square_row(mid)
    for d in FAR_FIRST:
        send(dss_s.at[0], dss_r.at[d - 1], 11, at_y(d))

    second = y % 3 == 0
    wait_bytes(w_r.at[0, pl.ds(0, 7)], recv_sem.at[8])
    wait_bytes(x_r.at[pl.ds(0, 7)], recv_sem.at[10])
    rows_in = dot_nt(keep, x_r[...].reshape(512, 128)).astype(BF16)
    d_s[0] = dot(rows_in, w_r[0].reshape(512, 256)).astype(BF16).reshape(8, 16, 256)
    for d in FAR_FIRST:
        send(d_s.at[0, (z + d) % RING], d_r.at[0, d - 1], 12, at_z(d))

    @pl.when(second)
    def _():
        wait_bytes(w_r.at[1, pl.ds(0, 7)], recv_sem.at[9])
        d_s[1] = dot(rows_in, w_r[1].reshape(512, 256)).astype(BF16).reshape(8, 16, 256)
        for d in FAR_FIRST:
            send(d_s.at[1, (z + d) % RING], d_r.at[1, d - 1], 13, at_z(d))

    for d in FAR_FIRST:
        send(wdt_v.at[(y + d) % RING], v_r.at[0, y], 18, at_y(d))

        @pl.when((y + d) % RING % 3 == 0)
        def _(d=d):
            send(wdt_v.at[8 + (y + d) % RING // 3], v_r.at[1, y], 19, at_y(d))

    wait_bytes(dss_r, recv_sem.at[11])
    ss = dss_s[0]
    for n in range(7):
        ss = ss + dss_r[n]
    dss2_s[0] = ss
    for d in FAR_FIRST:
        send(dss2_s.at[0], dss2_r.at[d - 1], 14, at_z(d))
    wait_bytes(dss2_r, recv_sem.at[14])
    for n in range(7):
        ss = ss + dss2_r[n]
    ffn_rms = lax.rsqrt(column_of(ss, 16 * z, 16) / 4096.0 + EPS)

    def finish(slot):
        wait_bytes(d_r.at[slot], recv_sem.at[12 + slot])
        total = d_s[slot, z].astype(F32)
        for n in range(7):
            total = total + d_r[slot, n].astype(F32)
        total = total * ffn_rms
        hidden = (silu(total[:, 0:128]) * total[:, 128:256]).astype(BF16)
        e_s[slot] = hidden
        e_r[slot, z] = hidden
        for d in FAR_FIRST:
            send(e_s.at[slot], e_r.at[slot, z], 15 + slot, at_z(d))

    @pl.when(second)
    def _():
        finish(1)

    finish(0)

    def down(slot):
        wait_bytes(e_r.at[slot, pl.ds(0, 7)], recv_sem.at[15 + slot])
        wait_bytes(v_r.at[slot, pl.ds(0, 7)], recv_sem.at[18 + slot])
        return dot_nt(v_r[slot].reshape(512, 128), e_r[slot].reshape(128, 128))

    @pl.when(second)
    def _():
        g_s[...] = (down(1) + down(0)).astype(BF16).reshape(8, 64, 128)

    @pl.when(jnp.logical_not(second))
    def _():
        g_s[...] = down(0).astype(BF16).reshape(8, 64, 128)

    for d in FAR_FIRST:
        send(g_s.at[(y + d) % RING], g_r.at[d - 1], 20, at_y(d))
    wait_bytes(g_r, recv_sem.at[20])
    partial = g_s[y].astype(F32)
    for n in range(7):
        partial = partial + g_r[n].astype(F32)
    partial = partial.astype(BF16)
    f_s[0] = partial
    f_r[tp] = partial
    for d in (4, 3, 5, 2, 6, 1, 7):
        send(f_s.at[0], f_r.at[tp], 17, at_tp(d))
    wait_bytes(f_r.at[pl.ds(0, 7)], recv_sem.at[17])
    ffn_out = f_r[0].astype(F32)
    for n in range(1, 8):
        ffn_out = ffn_out + f_r[n].astype(F32)
    mixed_o[...] = (mid + ffn_out).astype(BF16)

    seven = pl.ds(0, 7)
    drains = (
        az_r, ay_r, ass_r, az2_r, ay2_r, ass2_r, b_r.at[pl.ds(0, 63)], c_r.at[seven], w_r.at[0, seven], None,
        x_r.at[seven], dss_r, d_r.at[0], None, dss2_r, e_r.at[0, seven], None, f_r.at[seven],
        v_r.at[0, seven], None, g_r,
    )
    for slot, ref in enumerate(drains):
        if ref is not None:
            wait_bytes(ref, send_sem.at[slot])

    @pl.when(second)
    def _():
        wait_bytes(d_r.at[1], send_sem.at[13])
        wait_bytes(e_r.at[1, seven], send_sem.at[16])

    for d in FAR_FIRST:

        @pl.when((y + d) % RING % 3 == 0)
        def _():
            wait_bytes(w_r.at[1, pl.ds(0, 1)], send_sem.at[9])
            wait_bytes(v_r.at[1, pl.ds(0, 1)], send_sem.at[19])


def store(mixed_v, state_v, mixed_h, state_h, sem):
    copies = (
        pltpu.make_async_copy(state_v, state_h, sem.at[0]),
        pltpu.make_async_copy(mixed_v, mixed_h, sem.at[1]),
    )
    for copy in copies:
        copy.start()
    for copy in copies:
        copy.wait()


def local(
    tokens, mix_gain, ffn_gain, w_query, w_key, w_value, w_gate, w_decay, decay_bias, head_gain,
    w_output, w_ffgate, w_ffup, w_down, state,
):
    hidden_units = w_ffgate.shape[1]
    V = pltpu.VMEM
    scratch = [
        V((64, 128), BF16), V((1, 64), BF16), V((1, 64), BF16), V((64, 896), BF16), V((64, 896), BF16),
        V((1, 256), F32), V((512,), BF16), V((64, 512), BF16), V((64, hidden_units), BF16),
        V((64, hidden_units), BF16), V((64, hidden_units), BF16),
        V((UNITS, 64, 256), BF16), V((UNITS, 64, 128), BF16),
        V((8, 16, 896), BF16), V((7, 16, 896), BF16), V((8, 16, 896), BF16), V((7, 16, 896), BF16),
        V((8, 2, 896), BF16), V((7, 2, 896), BF16), V((8, 2, 896), BF16), V((7, 2, 896), BF16),
        V((1, 1, 128), F32), V((7, 1, 128), F32), V((1, 1, 128), F32), V((7, 1, 128), F32),
        V((1, 2, 512), BF16), V((64, 2, 512), BF16), V((1, 64, 128), BF16), V((8, 64, 128), BF16),
        V((2, 8, 64, 256), BF16), V((1, 64, 128), BF16), V((8, 64, 128), BF16),
        V((2, 8, 16, 256), BF16), V((2, 7, 16, 256), BF16),
        V((1, 1, 128), F32), V((7, 1, 128), F32), V((1, 1, 128), F32), V((7, 1, 128), F32),
        V((2, 8, 64, 128), BF16), V((2, 16, 128), BF16), V((2, 8, 16, 128), BF16), V((8, 64, 128), BF16), V((7, 64, 128), BF16), V((1, 64, 128), BF16), V((8, 64, 128), BF16),
        pltpu.SemaphoreType.DMA((16,)),
        pltpu.SemaphoreType.DMA((21,)), pltpu.SemaphoreType.DMA((21,)),
    ]
    operands = (
        tokens.T, mix_gain.reshape(1, 64), ffn_gain.reshape(1, 64), w_query, w_key, w_value, w_gate, w_decay,
        decay_bias.reshape(1, 256), head_gain, w_output.T, w_ffgate, w_ffup, w_down.T, state.reshape(2, 256, 512),
    )
    mixed, new_state = pl.pallas_call(
        kernel,
        name="layer",
        out_shape=(
            jax.ShapeDtypeStruct((64, 128), BF16),
            jax.ShapeDtypeStruct((2, 256, 512), F32),
        ),
        in_specs=[pl.BlockSpec(memory_space=pltpu.HBM)] * 15,
        out_specs=[pl.BlockSpec(memory_space=pltpu.VMEM)] * 2,
        scratch_shapes=scratch,
        compiler_params=pltpu.CompilerParams(
            collective_id=0, has_side_effects=True, vmem_limit_bytes=40000000
        ),
    )(*[pltpu.with_memory_space_constraint(a, pltpu.HBM) for a in operands])
    mixed, new_state = pl.pallas_call(
        store,
        name="store",
        out_shape=(jax.ShapeDtypeStruct((64, 128), BF16), jax.ShapeDtypeStruct((2, 256, 512), F32)),
        in_specs=[pl.BlockSpec(memory_space=pltpu.VMEM)] * 2,
        out_specs=[pl.BlockSpec(memory_space=pltpu.HBM)] * 2,
        scratch_shapes=[pltpu.SemaphoreType.DMA((2,))],
        compiler_params=pltpu.CompilerParams(vmem_limit_bytes=40000000),
    )(mixed, new_state)
    new_state = new_state.reshape(2, 1, 256, 512)
    return (mixed.T, new_state)


def solution(mesh):
    in_specs = (
        P(None, "kv"),
        P("kv"),
        P("kv"),
        P("kv", "tp"),
        P("kv", "tp"),
        P("kv", "tp"),
        P("kv", "tp"),
        P("kv", "tp"),
        P("tp"),
        P(),
        P("tp", "kv"),
        P("kv", "tp"),
        P("kv", "tp"),
        P("tp", "kv"),
        P("kv", "tp", None, None),
    )
    out_specs = (P(None, "kv"), P("kv", "tp", None, None))
    return jax.shard_map(local, mesh=mesh, in_specs=in_specs, out_specs=out_specs, check_vma=False)
```

```python
import jax
import jax.numpy as jnp
from jax import lax
from jax.experimental import pallas as pl
from jax.experimental.pallas import tpu as pltpu
from jax.sharding import PartitionSpec as P

MESH = pl.DeviceIdType.MESH
EPS = 1e-06
F32 = jnp.float32
BF16 = jnp.bfloat16
RING = 8
FAR_FIRST = (4, 3, 5, 2, 6, 1, 7)
UNITS = 11
SPREAD = sorted(
    ((dz, dy) for dz in range(RING) for dy in range(RING) if dz + dy > 0),
    key=lambda t: -min(t[0], RING - t[0]) - min(t[1], RING - t[1]),
)


def far(k):
    odd = k % 2
    return (4 + (k // 2) * (1 - odd) - ((k + 1) // 2) * odd + RING) % RING


def wait_bytes(ref, sem):
    pltpu.make_async_copy(ref, ref, sem).wait()


def silu(v):
    return v / (1.0 + jnp.exp(-v))


def dot(a, b):
    return jnp.dot(a, b, preferred_element_type=F32)


def dot_nt(a, b):
    return lax.dot_general(a, b, (((1,), (1,)), ((), ())), preferred_element_type=F32)


def square_row(x):
    squares = x * x
    high = squares.astype(BF16)
    low = (squares - high.astype(F32)).astype(BF16)
    ones = jnp.ones((8, x.shape[0]), BF16)
    return (dot(ones, high) + dot(ones, low))[0:1, :]


def column_of(row, first, count):
    lane = lax.broadcasted_iota(jnp.int32, (count, row.shape[1]), 1)
    place = lax.broadcasted_iota(jnp.int32, (count, row.shape[1]), 0) + first
    return jnp.sum(jnp.where(lane == place, row, 0.0), axis=1, keepdims=True)


def kernel(
    tokens_h, mix_gain_h, ffn_gain_h, wq_h, wk_h, wv_h, wg_h, wd_h, bias_h, head_gain_h,
    wo_h, wfg_h, wfu_h, wdn_h, state_h,
    mixed_o, state_v,
    tokens_v, mix_gain_v, ffn_gain_v, w1_v, w2_v, bias_v, head_gain_v, wo_v, wfg_v, wfu_v, wdn_v,
    wgu_v, wdt_v,
    az_s, az_r, ay_s, ay_r, az2_s, az2_r, ay2_s, ay2_r, ass_s, ass_r, ass2_s, ass2_r,
    b_s, b_r, c_s, c_r,
    w_r, x_s, x_r, d_s, d_r, dss_s, dss_r, dss2_s, dss2_r,
    v_r, e_s, e_r, g_s, g_r, f_s, f_r,
    in_sem, send_sem, recv_sem,
):
    kv = lax.axis_index("kv")
    tp = lax.axis_index("tp")
    z = kv // RING
    y = kv % RING

    def at_z(d):
        return {"kv": ((z + d) % RING) * RING + y, "tp": tp}

    def at_y(d):
        return {"kv": z * RING + (y + d) % RING, "tp": tp}

    def at_tp(d):
        return {"kv": kv, "tp": (tp + d) % 8}

    def send(src, dst, slot, peer):
        pltpu.make_async_remote_copy(
            src_ref=src, dst_ref=dst, send_sem=send_sem.at[slot], recv_sem=recv_sem.at[slot],
            device_id=peer, device_id_type=MESH,
        ).start()

    loads = [
        (tokens_h, tokens_v), (mix_gain_h, mix_gain_v),
        (wq_h, w1_v.at[:, 0:256]), (wk_h, w1_v.at[:, 256:512]), (wd_h, w1_v.at[:, 512:768]),
        (wv_h.at[:, 0:128], w1_v.at[:, 768:896]), (wv_h.at[:, 128:512], w2_v.at[:, 0:384]),
        (wg_h, w2_v.at[:, 384:896]),
        (state_h, state_v), (bias_h, bias_v), (head_gain_h, head_gain_v), (ffn_gain_h, ffn_gain_v),
        (wo_h, wo_v), (wfg_h, wfg_v), (wfu_h, wfu_v), (wdn_h, wdn_v),
    ]
    copies = [pltpu.make_async_copy(src, dst, in_sem.at[n]) for n, (src, dst) in enumerate(loads)]
    for copy in copies:
        copy.start()
    barrier = pltpu.get_barrier_semaphore()
    for d in FAR_FIRST:
        for peer in (at_z(d), at_y(d), at_tp(d)):
            pl.semaphore_signal(barrier, inc=1, device_id=peer, device_id_type=MESH)

    for copy in copies[:6]:
        copy.wait()

    token_f32 = tokens_v[...].astype(F32)
    mix_t = (token_f32 * column_of(mix_gain_v[...].astype(F32), 0, 64)).astype(BF16)
    row = lax.broadcasted_iota(jnp.int32, (128, 128), 0)
    col = lax.broadcasted_iota(jnp.int32, (128, 128), 1)
    keep = jnp.where(col == row, 1.0, 0.0).astype(BF16)
    by_y = 16 * ((row % 16) // 2) + 2 * (row // 16) + row % 2
    shuffle = jnp.where(col == by_y, 1.0, 0.0).astype(BF16)
    mix_in = dot_nt(keep, mix_t).astype(BF16)
    az_s[...] = dot(mix_in, w1_v[...]).astype(BF16).reshape(az_s.shape)
    ass_s[0] = square_row(token_f32)

    for copy in copies[6:8]:
        copy.wait()
    mix_by_y = dot_nt(shuffle, mix_t).astype(BF16)
    ay_s[...] = dot(mix_by_y, w2_v[...]).astype(BF16).reshape(ay_s.shape)
    pl.semaphore_wait(barrier, 21)
    for d in FAR_FIRST:
        send(ass_s.at[0], ass_r.at[d - 1], 2, at_z(d))
    for d in FAR_FIRST:
        send(az_s.at[(z + d) % RING], az_r.at[d - 1], 0, at_z(d))
        send(ay_s.at[(y + d) % RING], ay_r.at[d - 1], 1, at_y(d))

    for copy in copies[8:]:
        copy.wait()
    for u in range(UNITS):
        for side, ref in enumerate((wfg_v, wfu_v, wdn_v)):
            width = min(128, ref.shape[1] - 128 * u)
            part = ref[:, 128 * u : 128 * u + width]
            if width < 128:
                part = jnp.concatenate([part, jnp.zeros((64, 128 - width), BF16)], axis=1)
            if side < 2:
                wgu_v[u, :, 128 * side : 128 * side + 128] = part
            else:
                wdt_v[u] = part
    w_r[0, y] = wgu_v[y]
    w_r[1, y] = wgu_v[8 + y // 3]
    v_r[0, y] = wdt_v[y]
    v_r[1, y] = wdt_v[8 + y // 3]

    wait_bytes(az_r, recv_sem.at[0])
    by_z = az_s[z].astype(F32)
    for n in range(7):
        by_z = by_z + az_r[n].astype(F32)
    by_z = by_z.astype(BF16)
    for n in range(RING):
        az2_s[n] = by_z[2 * n : 2 * n + 2, :]
    wait_bytes(ass_r, recv_sem.at[2])
    ss = ass_s[0]
    for n in range(7):
        ss = ss + ass_r[n]
    ass2_s[0] = ss
    for d in FAR_FIRST:
        send(az2_s.at[(y + d) % RING], az2_r.at[d - 1], 3, at_y(d))
        send(ass2_s.at[0], ass2_r.at[d - 1], 5, at_y(d))
    wait_bytes(ay_r, recv_sem.at[1])
    by_y = ay_s[y].astype(F32)
    for n in range(7):
        by_y = by_y + ay_r[n].astype(F32)
    by_y = by_y.astype(BF16)
    for n in range(RING):
        ay2_s[n] = by_y[2 * n : 2 * n + 2, :]
    for d in FAR_FIRST:
        send(ay2_s.at[(z + d) % RING], ay2_r.at[d - 1], 4, at_z(d))
    for d in FAR_FIRST:
        send(wgu_v.at[(y + d) % RING], w_r.at[0, y], 8, at_y(d))

    wait_bytes(az2_r, recv_sem.at[3])
    wait_bytes(ay2_r, recv_sem.at[4])
    wait_bytes(ass2_r, recv_sem.at[5])
    left = az2_s[y].astype(F32)
    right = ay2_s[z].astype(F32)
    ss = ass2_s[0]
    for n in range(7):
        left = left + az2_r[n].astype(F32)
        right = right + ay2_r[n].astype(F32)
        ss = ss + ass2_r[n]
    mix_rms = lax.rsqrt(column_of(ss, 2 * kv, 2) / 4096.0 + EPS)
    left = left * mix_rms
    right = right * mix_rms
    queries = left[:, 0:256] * (256.0 ** -0.5)
    keys = left[:, 256:512]
    raw_decay = left[:, 512:768] + bias_v[...]
    log_decay = (jnp.minimum(raw_decay, 0.0) - jnp.log1p(jnp.exp(-jnp.abs(raw_decay)))) / 16.0
    decay = jnp.exp(log_decay)
    values = jnp.concatenate([left[:, 768:896], right[:, 0:384]], axis=1)
    gates = right[:, 384:896]
    columns = jnp.concatenate([decay, keys, queries, queries], axis=0).T
    outs = []
    for s in range(2):
        value = values[s : s + 1, :]
        total = jnp.zeros((8, 512), F32)
        for block in range(8):
            rows = slice(32 * block, 32 * block + 32)
            fresh = columns[rows, s : s + 1] * state_v[s, rows, :] + columns[rows, 2 + s : 3 + s] * value
            state_v[s, rows, :] = fresh
            weighted = columns[rows, 4 + s : 5 + s] * fresh
            total = total + weighted[0:8] + weighted[8:16] + weighted[16:24] + weighted[24:32]
        outs.append(jnp.sum(total, axis=0, keepdims=True))
    attended = jnp.concatenate(outs, axis=0)
    attended = attended * lax.rsqrt(jnp.sum(attended * attended, axis=1, keepdims=True) / 512.0 + EPS)
    head_out = (attended * head_gain_v[...].astype(F32)[None, :] * silu(gates)).astype(BF16)
    b_s[0] = head_out
    b_r[kv] = head_out

    for dz, dy in SPREAD:
        peer = ((z + dz) % RING) * RING + (y + dy) % RING
        send(b_s.at[0], b_r.at[kv], 6, {"kv": peer, "tp": tp})
    wait_bytes(b_r.at[pl.ds(0, 63)], recv_sem.at[6])
    heads = b_r[...].reshape(128, 512)
    partial = dot_nt(wo_v[...], heads).astype(BF16)
    c_s[0] = partial
    c_r[tp] = partial
    for d in (4, 3, 5, 2, 6, 1, 7):
        send(c_s.at[0], c_r.at[tp], 7, at_tp(d))
    for d in FAR_FIRST:

        @pl.when((y + d) % RING % 3 == 0)
        def _(d=d):
            send(wgu_v.at[8 + (y + d) % RING // 3], w_r.at[1, y], 9, at_y(d))

    gain_column = column_of(ffn_gain_v[...].astype(F32), 0, 64)
    wait_bytes(c_r.at[pl.ds(0, 7)], recv_sem.at[7])
    attn_out = c_r[0].astype(F32)
    for n in range(1, 8):
        attn_out = attn_out + c_r[n].astype(F32)
    mid = (token_f32 + attn_out).astype(BF16).astype(F32)
    ffn_in = (mid * gain_column).astype(BF16)
    dss_s[0] = square_row(mid)
    x_s[0] = ffn_in
    for d in FAR_FIRST:
        send(dss_s.at[0], dss_r.at[d - 1], 11, at_y(d))
    for d in FAR_FIRST:
        send(x_s.at[0], x_r.at[y], 10, at_y(d))
    x_r[y] = ffn_in

    second = y % 3 == 0
    wait_bytes(dss_r, recv_sem.at[11])
    ss = dss_s[0]
    for n in range(7):
        ss = ss + dss_r[n]
    dss2_s[0] = ss
    for d in FAR_FIRST:
        send(dss2_s.at[0], dss2_r.at[d - 1], 14, at_z(d))
    wait_bytes(w_r.at[0, pl.ds(0, 7)], recv_sem.at[8])
    wait_bytes(x_r.at[pl.ds(0, 7)], recv_sem.at[10])
    rows_in = dot_nt(keep, x_r[...].reshape(512, 128)).astype(BF16)
    d_s[0] = dot(rows_in, w_r[0].reshape(512, 256)).astype(BF16).reshape(8, 16, 256)
    for d in FAR_FIRST:
        send(d_s.at[0, (z + d) % RING], d_r.at[0, d - 1], 12, at_z(d))

    @pl.when(second)
    def _():
        wait_bytes(w_r.at[1, pl.ds(0, 7)], recv_sem.at[9])
        d_s[1] = dot(rows_in, w_r[1].reshape(512, 256)).astype(BF16).reshape(8, 16, 256)
        for d in FAR_FIRST:
            send(d_s.at[1, (z + d) % RING], d_r.at[1, d - 1], 13, at_z(d))

    for d in FAR_FIRST:
        send(wdt_v.at[(y + d) % RING], v_r.at[0, y], 18, at_y(d))

        @pl.when((y + d) % RING % 3 == 0)
        def _(d=d):
            send(wdt_v.at[8 + (y + d) % RING // 3], v_r.at[1, y], 19, at_y(d))

    wait_bytes(dss2_r, recv_sem.at[14])
    for n in range(7):
        ss = ss + dss2_r[n]
    ffn_rms = lax.rsqrt(column_of(ss, 16 * z, 16) / 4096.0 + EPS)

    def finish(slot):
        wait_bytes(d_r.at[slot], recv_sem.at[12 + slot])
        total = d_s[slot, z].astype(F32)
        for n in range(7):
            total = total + d_r[slot, n].astype(F32)
        total = total * ffn_rms
        hidden = (silu(total[:, 0:128]) * total[:, 128:256]).astype(BF16)
        e_s[slot] = hidden
        e_r[slot, z] = hidden
        for d in FAR_FIRST:
            send(e_s.at[slot], e_r.at[slot, z], 15 + slot, at_z(d))

    @pl.when(second)
    def _():
        finish(1)

    finish(0)

    def down(slot):
        wait_bytes(e_r.at[slot, pl.ds(0, 7)], recv_sem.at[15 + slot])
        wait_bytes(v_r.at[slot, pl.ds(0, 7)], recv_sem.at[18 + slot])
        return dot_nt(v_r[slot].reshape(512, 128), e_r[slot].reshape(128, 128))

    @pl.when(second)
    def _():
        g_s[...] = (down(1) + down(0)).astype(BF16).reshape(8, 64, 128)

    @pl.when(jnp.logical_not(second))
    def _():
        g_s[...] = down(0).astype(BF16).reshape(8, 64, 128)

    for d in FAR_FIRST:
        send(g_s.at[(y + d) % RING], g_r.at[d - 1], 20, at_y(d))
    wait_bytes(g_r, recv_sem.at[20])
    partial = g_s[y].astype(F32)
    for n in range(7):
        partial = partial + g_r[n].astype(F32)
    partial = partial.astype(BF16)
    f_s[0] = partial
    f_r[tp] = partial
    for d in (4, 3, 5, 2, 6, 1, 7):
        send(f_s.at[0], f_r.at[tp], 17, at_tp(d))
    wait_bytes(f_r.at[pl.ds(0, 7)], recv_sem.at[17])
    ffn_out = f_r[0].astype(F32)
    for n in range(1, 8):
        ffn_out = ffn_out + f_r[n].astype(F32)
    mixed_o[...] = (mid + ffn_out).astype(BF16)

    seven = pl.ds(0, 7)
    drains = (
        az_r, ay_r, ass_r, az2_r, ay2_r, ass2_r, b_r.at[pl.ds(0, 63)], c_r.at[seven], w_r.at[0, seven], None,
        x_r.at[seven], dss_r, d_r.at[0], None, dss2_r, e_r.at[0, seven], None, f_r.at[seven],
        v_r.at[0, seven], None, g_r,
    )
    for slot, ref in enumerate(drains):
        if ref is not None:
            wait_bytes(ref, send_sem.at[slot])

    @pl.when(second)
    def _():
        wait_bytes(d_r.at[1], send_sem.at[13])
        wait_bytes(e_r.at[1, seven], send_sem.at[16])

    for d in FAR_FIRST:

        @pl.when((y + d) % RING % 3 == 0)
        def _():
            wait_bytes(w_r.at[1, pl.ds(0, 1)], send_sem.at[9])
            wait_bytes(v_r.at[1, pl.ds(0, 1)], send_sem.at[19])


def store(mixed_v, state_v, mixed_h, state_h, sem):
    copies = (
        pltpu.make_async_copy(state_v, state_h, sem.at[0]),
        pltpu.make_async_copy(mixed_v, mixed_h, sem.at[1]),
    )
    for copy in copies:
        copy.start()
    for copy in copies:
        copy.wait()


def local(
    tokens, mix_gain, ffn_gain, w_query, w_key, w_value, w_gate, w_decay, decay_bias, head_gain,
    w_output, w_ffgate, w_ffup, w_down, state,
):
    hidden_units = w_ffgate.shape[1]
    V = pltpu.VMEM
    scratch = [
        V((64, 128), BF16), V((1, 64), BF16), V((1, 64), BF16), V((64, 896), BF16), V((64, 896), BF16),
        V((1, 256), F32), V((512,), BF16), V((64, 512), BF16), V((64, hidden_units), BF16),
        V((64, hidden_units), BF16), V((64, hidden_units), BF16),
        V((UNITS, 64, 256), BF16), V((UNITS, 64, 128), BF16),
        V((8, 16, 896), BF16), V((7, 16, 896), BF16), V((8, 16, 896), BF16), V((7, 16, 896), BF16),
        V((8, 2, 896), BF16), V((7, 2, 896), BF16), V((8, 2, 896), BF16), V((7, 2, 896), BF16),
        V((1, 1, 128), F32), V((7, 1, 128), F32), V((1, 1, 128), F32), V((7, 1, 128), F32),
        V((1, 2, 512), BF16), V((64, 2, 512), BF16), V((1, 64, 128), BF16), V((8, 64, 128), BF16),
        V((2, 8, 64, 256), BF16), V((1, 64, 128), BF16), V((8, 64, 128), BF16),
        V((2, 8, 16, 256), BF16), V((2, 7, 16, 256), BF16),
        V((1, 1, 128), F32), V((7, 1, 128), F32), V((1, 1, 128), F32), V((7, 1, 128), F32),
        V((2, 8, 64, 128), BF16), V((2, 16, 128), BF16), V((2, 8, 16, 128), BF16), V((8, 64, 128), BF16), V((7, 64, 128), BF16), V((1, 64, 128), BF16), V((8, 64, 128), BF16),
        pltpu.SemaphoreType.DMA((16,)),
        pltpu.SemaphoreType.DMA((21,)), pltpu.SemaphoreType.DMA((21,)),
    ]
    operands = (
        tokens.T, mix_gain.reshape(1, 64), ffn_gain.reshape(1, 64), w_query, w_key, w_value, w_gate, w_decay,
        decay_bias.reshape(1, 256), head_gain, w_output.T, w_ffgate, w_ffup, w_down.T, state.reshape(2, 256, 512),
    )
    mixed, new_state = pl.pallas_call(
        kernel,
        name="layer",
        out_shape=(
            jax.ShapeDtypeStruct((64, 128), BF16),
            jax.ShapeDtypeStruct((2, 256, 512), F32),
        ),
        in_specs=[pl.BlockSpec(memory_space=pltpu.HBM)] * 15,
        out_specs=[pl.BlockSpec(memory_space=pltpu.VMEM)] * 2,
        scratch_shapes=scratch,
        compiler_params=pltpu.CompilerParams(
            collective_id=0, has_side_effects=True, vmem_limit_bytes=40000000
        ),
    )(*[pltpu.with_memory_space_constraint(a, pltpu.HBM) for a in operands])
    mixed, new_state = pl.pallas_call(
        store,
        name="store",
        out_shape=(jax.ShapeDtypeStruct((64, 128), BF16), jax.ShapeDtypeStruct((2, 256, 512), F32)),
        in_specs=[pl.BlockSpec(memory_space=pltpu.VMEM)] * 2,
        out_specs=[pl.BlockSpec(memory_space=pltpu.HBM)] * 2,
        scratch_shapes=[pltpu.SemaphoreType.DMA((2,))],
        compiler_params=pltpu.CompilerParams(vmem_limit_bytes=40000000),
    )(mixed, new_state)
    new_state = new_state.reshape(2, 1, 256, 512)
    return (mixed.T, new_state)


def solution(mesh):
    in_specs = (
        P(None, "kv"),
        P("kv"),
        P("kv"),
        P("kv", "tp"),
        P("kv", "tp"),
        P("kv", "tp"),
        P("kv", "tp"),
        P("kv", "tp"),
        P("tp"),
        P(),
        P("tp", "kv"),
        P("kv", "tp"),
        P("kv", "tp"),
        P("tp", "kv"),
        P("kv", "tp", None, None),
    )
    out_specs = (P(None, "kv"), P("kv", "tp", None, None))
    return jax.shard_map(local, mesh=mesh, in_specs=in_specs, out_specs=out_specs, check_vma=False)
```
